32 devices in a mesh: grp: 2 (over x), tp: 4 (over z), dp: 4 (over y, core).
Axes of the slice: x: 2, y: 2, z: 4, core: 2. Of those that a mesh axis runs over, the one named last changes fastest.
Arguments:
- hidden: bfloat16 [16, 2048], P('grp', 'dp'), parts along dimension 0, may hold values from -20 to 20
- lengths: int32 [16], P(('grp', 'dp')), parts along dimension 0, may hold values from 1 to 256, 512 in all
- input_norm_gain: float32 [2, 2048], P(None, 'dp'), may hold values from 0.1 to 1.9
- gate_matrix: bfloat16 [2, 2048, 4096], P(None, 'dp', 'tp'), may hold values from -0.125 to 0.125
- input_matrix: bfloat16 [2, 2048, 4096], P(None, 'dp', 'tp'), may hold values from -0.125 to 0.125
- write_matrix: bfloat16 [2, 2048, 2048], P(None, 'dp', 'tp'), may hold values from -0.125 to 0.125
- read_matrix: bfloat16 [2, 2048, 2048], P(None, 'dp', 'tp'), may hold values from -0.125 to 0.125
- step_matrix: bfloat16 [2, 2048, 64], P(None, 'dp'), may hold values from -0.125 to 0.125
- step_size_bias: float32 [2, 64], P(None, 'tp'), may hold values from -2 to 1
- log_decay_rate: float32 [2, 64], P(None, 'tp'), may hold values from -1 to 2
- direct_path_gain: float32 [2, 64], P(None, 'tp'), may hold values from 0.5 to 1.5
- input_filter_taps: bfloat16 [2, 4, 4096], P(None, None, 'tp'), may hold values from -3 to 3
- write_filter_taps: bfloat16 [2, 4, 2048], P(None, None, 'tp'), may hold values from -3 to 3
- read_filter_taps: bfloat16 [2, 4, 2048], P(None, None, 'tp'), may hold values from -3 to 3
- position_log_decay: float32 [2, 256, 64], P(None, None, 'tp'), may hold values from -0.7 to 0
- grouped_norm_gain: float32 [2, 4096], P(None, 'tp'), may hold values from 0.1 to 1.9
- output_matrix: bfloat16 [2, 4096, 2048], P(None, 'tp', 'dp'), may hold values from -0.09375 to 0.09375
- recurrent_head_state: float32 [2, 16, 64, 64, 128], P(None, ('grp', 'dp'), 'tp'), parts along dimension 1, may hold values from -3 to 3
- history_input_rows: bfloat16 [2, 16, 3, 4096], P(None, ('grp', 'dp'), None, 'tp'), parts along dimension 1, may hold values from -5 to 5
- history_write_rows: bfloat16 [2, 16, 3, 2048], P(None, ('grp', 'dp'), None, 'tp'), parts along dimension 1, may hold values from -5 to 5
- history_read_rows: bfloat16 [2, 16, 3, 2048], P(None, ('grp', 'dp'), None, 'tp'), parts along dimension 1, may hold values from -5 to 5
Outputs:
- stream_out: bfloat16 [16, 2048], P('grp', 'dp'), parts along dimension 0
- state_out: float32 [2, 16, 64, 64, 128], P(None, ('grp', 'dp'), 'tp'), parts along dimension 1
- buffer_value_out: bfloat16 [2, 16, 3, 4096], P(None, ('grp', 'dp'), None, 'tp'), parts along dimension 1
- buffer_write_out: bfloat16 [2, 16, 3, 2048], P(None, ('grp', 'dp'), None, 'tp'), parts along dimension 1
- buffer_read_out: bfloat16 [2, 16, 3, 2048], P(None, ('grp', 'dp'), None, 'tp'), parts along dimension 1
The draws below stay inside these ranges and needn't reach their ends.
There are 2 independent parts, one for each index of `grp`. The reference program is written for one: setup_inputs(seed, part) draws one part's arguments, and reference() takes and returns one part's arrays. A program takes and returns all parts, laid end to end along the dimension named above; an argument that names none is the same for every part. Nothing has to cross between parts.
Inputs may be any that keep to these rules, and one draw needn't show every extreme that they name: `lengths`: a sequence's current token stands at position length - 1; some sequence has length 256.
All inputs are finite; a program needn't handle non-finite values. No bound on the sum of `lengths` on one device may be relied on, other than what follows from the above.
Results may differ from the reference program's by a relative error of at most 0.0065.
Values may be sent and summed in bfloat16 or wider, within the bound.
No kernel may reach another device: no remote copies, remote signals or barrier semaphores. Data moves between devices by JAX's collectives and lax.ppermute only.
A program may use at most 64 MiB of HBM per device.

```python
import math
import jax
import jax.numpy as jnp
import numpy as np
from jax import lax

D = 2048
MIXER_HEADS = 64
HEAD_DIM = 64
GROUPS = 16
STATE = 128
TAPS = 4
MIXER_LAYERS = 2
LONGEST_LENGTH = 256
MEAN_LEN = 64
SEQS = 8
INNER = 4096


def draw_hidden(key, part):
    base_key = jax.random.fold_in(key, 17)
    row_key, entry_key = jax.random.split(base_key, 2)
    row_scales = jnp.exp(jax.random.uniform(row_key, (SEQS, 1), jnp.float32, math.log(0.3), math.log(3.0)))
    column_scales = jnp.exp(math.log(0.6) + math.log(3.0) * jnp.arange(D, dtype=jnp.float32) / D)[None, :]
    values = jnp.clip(jax.random.normal(entry_key, (SEQS, D), jnp.float32), -3.0, 3.0)
    return (values * row_scales * column_scales).astype(jnp.bfloat16)


def levels(key, dims, shards, least, high):
    def one(position, blocks):
        heights = jax.random.uniform(jax.random.fold_in(jax.random.fold_in(key, 6), position), (blocks,), jnp.float32, least / len(shards), high / len(shards))
        return jnp.repeat(jnp.exp(heights), dims[position] // blocks).reshape((-1,) + (1,) * (len(dims) - position - 1))

    factor_of = one(*shards[0])
    for cut in shards[1:]:
        factor_of = factor_of * one(*cut)
    return factor_of


def split_up(amount, total, limit, slope):
    weights = [(1 << 20) // math.isqrt(standing ** slope) + 1 for standing in range(2, amount + 1)]
    surplus, counts = total - limit - (amount - 1), [1] * (amount - 1)
    while surplus > 0:
        movable = [i for i in range(amount - 1) if counts[i] < limit]
        whole, left = sum([weights[i] for i in movable]), surplus
        for i in movable:
            extra = min(limit - counts[i], max(1, left * weights[i] // whole), surplus)
            counts[i] = counts[i] + extra
            surplus = surplus - extra
    return np.array([limit] + counts)


def uneven(key, count, total, limit, skew):
    if count == 2:
        one = jax.random.randint(key, (), max(1, total - limit), min(limit, total - 1) + 1)
        return jnp.stack([one, total - one])
    sizes = jnp.asarray(split_up(count, total, limit, skew), jnp.int32)
    couples = (count - 1) // 2
    donor, sink = sizes[1:1 + 2 * couples:2], sizes[2:2 + 2 * couples:2]
    room = jnp.minimum(donor - 1, limit - sink)
    moved = jax.random.randint(jax.random.fold_in(key, 1), (couples,), 0, 1 << 20) % (room + 1)
    sizes = sizes.at[1:1 + 2 * couples:2].set(donor - moved).at[2:2 + 2 * couples:2].set(sink + moved)
    return sizes[jax.random.permutation(jax.random.fold_in(key, 2), count)]


def normal_values(own_key, extent, spread, reach, pieces=(), kind=jnp.bfloat16):
    level = levels(own_key, extent, pieces, -0.22, 0.18) if pieces else 1.0
    entries = jax.random.normal(own_key, extent, jnp.float32) * spread * level
    return jnp.minimum(jnp.maximum(entries, -reach), reach).astype(kind)


def setup_inputs(seed: int = 0, part: int = 0) -> dict:
    splits = jax.random.split(jax.random.key(seed), 22)
    part_splits = jax.random.split(jax.random.fold_in(splits[21], part), 22)
    hidden = draw_hidden(jax.random.fold_in(jax.random.fold_in(splits[21], part), 71), part)
    lengths = uneven(part_splits[1], SEQS, SEQS * MEAN_LEN, LONGEST_LENGTH, 2).astype(jnp.int32)
    input_norm_gain = jnp.clip(1.0 + 0.18 * jax.random.normal(splits[2], (MIXER_LAYERS, D), jnp.float32), 0.1, 1.9)
    gate_matrix = normal_values(splits[3], (MIXER_LAYERS, D, INNER), D ** -0.5, 0.125, ((1, 4), (2, 4)))
    input_matrix = normal_values(splits[4], (MIXER_LAYERS, D, INNER), D ** -0.5, 0.125, ((1, 4), (2, 4)))
    write_matrix = normal_values(splits[5], (MIXER_LAYERS, D, GROUPS * STATE), D ** -0.5, 0.125, ((1, 4), (2, 4)))
    read_matrix = normal_values(splits[6], (MIXER_LAYERS, D, GROUPS * STATE), D ** -0.5, 0.125, ((1, 4), (2, 4)))
    step_matrix = normal_values(splits[7], (MIXER_LAYERS, D, MIXER_HEADS), D ** -0.5, 0.125, ((1, 4),))
    step_size_bias = jnp.clip(-2.0 + 3.0 * jax.random.uniform(splits[8], (MIXER_LAYERS, MIXER_HEADS), jnp.float32) ** levels(splits[8], (MIXER_LAYERS, MIXER_HEADS), ((1, 4),), -0.2, 0.2), -2.0, 1.0)
    log_decay_rate = jnp.clip(-1.0 + 3.0 * jax.random.uniform(splits[9], (MIXER_LAYERS, MIXER_HEADS), jnp.float32) ** levels(splits[9], (MIXER_LAYERS, MIXER_HEADS), ((1, 4),), -0.2, 0.2), -1.0, 2.0)
    direct_path_gain = jnp.clip(0.5 + 1.0 * jax.random.uniform(splits[10], (MIXER_LAYERS, MIXER_HEADS), jnp.float32) ** levels(splits[10], (MIXER_LAYERS, MIXER_HEADS), ((1, 4),), -0.2, 0.2), 0.5, 1.5)
    input_filter_taps = normal_values(splits[11], (MIXER_LAYERS, TAPS, INNER), TAPS ** -0.5, 3.0, ((2, 4),))
    write_filter_taps = normal_values(splits[12], (MIXER_LAYERS, TAPS, GROUPS * STATE), TAPS ** -0.5, 3.0, ((2, 4),))
    read_filter_taps = normal_values(splits[13], (MIXER_LAYERS, TAPS, GROUPS * STATE), TAPS ** -0.5, 3.0, ((2, 4),))
    position_log_decay = jnp.clip(-0.7 + 0.7 * jax.random.uniform(splits[14], (MIXER_LAYERS, LONGEST_LENGTH, MIXER_HEADS), jnp.float32) ** levels(splits[14], (MIXER_LAYERS, LONGEST_LENGTH, MIXER_HEADS), ((2, 4),), -0.2, 0.2), -0.7, 0.0)
    grouped_norm_gain = jnp.clip(1.0 + 0.18 * jax.random.normal(splits[15], (MIXER_LAYERS, INNER), jnp.float32), 0.1, 1.9)
    output_matrix = normal_values(splits[16], (MIXER_LAYERS, INNER, D), INNER ** -0.5, 0.09375, ((1, 4), (2, 4)))
    recurrent_head_state = normal_values(part_splits[17], (MIXER_LAYERS, SEQS, MIXER_HEADS, HEAD_DIM, STATE), 0.5, 3.0, ((1, 4), (2, 4)), jnp.float32)
    history_input_rows = normal_values(part_splits[18], (MIXER_LAYERS, SEQS, TAPS - 1, INNER), 1.0, 5.0, ((1, 4), (3, 4)))
    history_write_rows = normal_values(part_splits[19], (MIXER_LAYERS, SEQS, TAPS - 1, GROUPS * STATE), 1.0, 5.0, ((1, 4), (3, 4)))
    history_read_rows = normal_values(part_splits[20], (MIXER_LAYERS, SEQS, TAPS - 1, GROUPS * STATE), 1.0, 5.0, ((1, 4), (3, 4)))
    return {"hidden": hidden, "lengths": lengths, "input_norm_gain": input_norm_gain, "gate_matrix": gate_matrix, "input_matrix": input_matrix, "write_matrix": write_matrix, "read_matrix": read_matrix, "step_matrix": step_matrix, "step_size_bias": step_size_bias, "log_decay_rate": log_decay_rate, "direct_path_gain": direct_path_gain, "input_filter_taps": input_filter_taps, "write_filter_taps": write_filter_taps, "read_filter_taps": read_filter_taps, "position_log_decay": position_log_decay, "grouped_norm_gain": grouped_norm_gain, "output_matrix": output_matrix, "recurrent_head_state": recurrent_head_state, "history_input_rows": history_input_rows, "history_write_rows": history_write_rows, "history_read_rows": history_read_rows}


epsilon = 1e-06

def convolve(buffer, new_row, weights, tap_valid):
    tap_rows = weights.astype(jnp.float32)
    summed = new_row.astype(jnp.float32) * tap_rows[TAPS - 1]
    for k in range(TAPS - 1):
        summed = summed + buffer[:, k].astype(jnp.float32) * tap_rows[k] * tap_valid[:, k:k + 1]
    shifted = jnp.concatenate([buffer[:, 1:], new_row[:, None]], axis=1)
    return (jax.nn.silu(summed), shifted)

def per_sequence(seq_items):
    state_row, decay_row, step_row, value_heads, write_heads, read_heads = seq_items
    updated = decay_row[:, None, None] * state_row + (step_row[:, None] * value_heads)[:, :, None] * write_heads[:, None, :]
    readout = jnp.einsum('hpn,hn->hp', updated, read_heads, precision=lax.Precision.HIGHEST)
    return (updated, readout)

def reference(hidden, lengths, input_norm_gain, gate_matrix, input_matrix, write_matrix, read_matrix, step_matrix, step_size_bias, log_decay_rate, direct_path_gain, input_filter_taps, write_filter_taps, read_filter_taps, position_log_decay, grouped_norm_gain, output_matrix, recurrent_head_state, history_input_rows, history_write_rows, history_read_rows):
    per_group = MIXER_HEADS // GROUPS
    token_position = lengths - 1
    tap_valid = (jnp.arange(TAPS - 1)[None, :] >= TAPS - 1 - token_position[:, None]).astype(jnp.float32)
    state_is_valid = (token_position > 0).astype(jnp.float32)[:, None]
    position_indicator = (token_position[:, None] == jnp.arange(LONGEST_LENGTH)[None, :]).astype(jnp.float32)
    stream = hidden
    states, values, writes, reads = ([], [], [], [])
    for layer_index in range(MIXER_LAYERS):
        stream_float = stream.astype(jnp.float32)
        row_scale = lax.rsqrt(lax.optimization_barrier(jnp.mean(stream_float * stream_float, axis=1)) + epsilon)[:, None]
        normed = (stream_float * input_norm_gain[layer_index]).astype(jnp.bfloat16)
        proj_gate = jnp.dot(normed, gate_matrix[layer_index], preferred_element_type=jnp.float32) * row_scale
        proj_value = jnp.dot(normed, input_matrix[layer_index], preferred_element_type=jnp.float32) * row_scale
        proj_write = jnp.dot(normed, write_matrix[layer_index], preferred_element_type=jnp.float32) * row_scale
        proj_read = jnp.dot(normed, read_matrix[layer_index], preferred_element_type=jnp.float32) * row_scale
        proj_step = jnp.dot(normed, step_matrix[layer_index], preferred_element_type=jnp.float32) * row_scale
        value_act, value_buf = convolve(history_input_rows[layer_index], proj_value.astype(jnp.bfloat16), input_filter_taps[layer_index], tap_valid)
        write_act, write_buf = convolve(history_write_rows[layer_index], proj_write.astype(jnp.bfloat16), write_filter_taps[layer_index], tap_valid)
        read_act, read_buf = convolve(history_read_rows[layer_index], proj_read.astype(jnp.bfloat16), read_filter_taps[layer_index], tap_valid)
        head_step_size = jax.nn.softplus(proj_step + step_size_bias[layer_index])
        current_log_decay = jnp.dot(position_indicator, position_log_decay[layer_index], precision=lax.Precision.HIGHEST)
        current_decay = jnp.exp(-jnp.exp(log_decay_rate[layer_index]) * head_step_size + current_log_decay) * state_is_valid
        value_heads = value_act.reshape(SEQS, MIXER_HEADS, HEAD_DIM)
        write_heads = jnp.repeat(write_act.reshape(SEQS, GROUPS, STATE), per_group, axis=1)
        read_heads = jnp.repeat(read_act.reshape(SEQS, GROUPS, STATE), per_group, axis=1)
        updated, readout = lax.map(per_sequence, (recurrent_head_state[layer_index], current_decay, head_step_size, value_heads, write_heads, read_heads))
        mixed_heads = (readout + direct_path_gain[layer_index][None, :, None] * value_heads) * jax.nn.silu(proj_gate.reshape(SEQS, MIXER_HEADS, HEAD_DIM))
        grouped = mixed_heads.reshape(SEQS, GROUPS, per_group * HEAD_DIM)
        grouped = grouped * lax.rsqrt(lax.optimization_barrier(jnp.mean(grouped * grouped, axis=2, keepdims=True)) + epsilon)
        gated_rows = (grouped.reshape(SEQS, INNER) * grouped_norm_gain[layer_index]).astype(jnp.bfloat16)
        branch = jnp.dot(gated_rows, output_matrix[layer_index], preferred_element_type=jnp.float32)
        stream = (stream_float + branch).astype(jnp.bfloat16)
        states.append(updated)
        values.append(value_buf)
        writes.append(write_buf)
        reads.append(read_buf)
    return (stream, jnp.stack(states), jnp.stack(values), jnp.stack(writes), jnp.stack(reads))
```

```python
import jax
import jax.numpy as jnp
from jax import lax
from jax.sharding import PartitionSpec as P

D = 2048


epsilon = 1e-06


def convolve(buffer, new_row, weights, tap_valid):
    tap_rows = weights.astype(jnp.float32)
    depth = weights.shape[0] - 1
    summed = new_row.astype(jnp.float32) * tap_rows[depth]
    for k in range(depth):
        summed = summed + buffer[:, k].astype(jnp.float32) * tap_rows[k] * tap_valid[:, k : k + 1]
    shifted = jnp.concatenate([buffer[:, 1:], new_row[:, None]], axis=1)
    return (jax.nn.silu(summed), shifted)


def spread_groups(rows, seq_local, groups_local, per_group, state_dim):
    grouped = rows.reshape(seq_local, groups_local, 1, state_dim)
    return jnp.broadcast_to(grouped, (seq_local, groups_local, per_group, state_dim)).reshape(
        seq_local, groups_local * per_group, state_dim
    )


def direct(axis):
    size = lax.axis_size(axis)
    return size <= 8 and size & (size - 1) == 0


def swap(array, axis, mask):
    return lax.ppermute(array, axis, [(i, i ^ mask) for i in range(lax.axis_size(axis))])


def tree_sum(parts):
    while len(parts) > 1:
        parts = [parts[i] + parts[i + 1] for i in range(0, len(parts), 2)]
    return parts[0]


def exchange_rows(rows, axis, count):
    if not direct(axis):
        return lax.psum_scatter(rows, axis, scatter_dimension=0, tiled=True)
    me = lax.axis_index(axis)
    parts = [
        lax.dynamic_slice_in_dim(rows, (me ^ mask) * count, count, 0)
        for mask in range(lax.axis_size(axis))
    ]
    return tree_sum([parts[0]] + [swap(parts[mask], axis, mask) for mask in range(1, len(parts))])


def gather_rows(rows, axis):
    if not direct(axis):
        return lax.all_gather(rows, axis, axis=0, tiled=True)
    me, size = lax.axis_index(axis), lax.axis_size(axis)
    parts = [rows] + [swap(rows, axis, mask) for mask in range(1, size)]
    whole = jnp.zeros((size,) + rows.shape, rows.dtype)
    for mask in range(size):
        whole = lax.dynamic_update_index_in_dim(whole, parts[mask], me ^ mask, 0)
    return whole.reshape((size * rows.shape[0],) + rows.shape[1:])


def sum_copies(rows, axis):
    if not direct(axis):
        return lax.psum(rows, axis)
    return tree_sum([rows] + [swap(rows, axis, mask) for mask in range(1, lax.axis_size(axis))])


def on_device(
    hidden,
    lengths,
    input_norm_gain,
    gate_matrix,
    input_matrix,
    write_matrix,
    read_matrix,
    step_matrix,
    step_size_bias,
    log_decay_rate,
    direct_path_gain,
    input_filter_taps,
    write_filter_taps,
    read_filter_taps,
    position_log_decay,
    grouped_norm_gain,
    output_matrix,
    recurrent_head_state,
    history_input_rows,
    history_write_rows,
    history_read_rows,
):
    seq_local = lengths.shape[0]
    heads_local = step_size_bias.shape[1]
    head_dim = recurrent_head_state.shape[3]
    state_dim = recurrent_head_state.shape[4]
    groups_local = write_filter_taps.shape[2] // state_dim
    per_group = heads_local // groups_local
    inner_local = heads_local * head_dim
    shared_local = groups_local * state_dim
    depth = input_filter_taps.shape[1] - 1
    token_position = lengths - 1
    tap_valid = (jnp.arange(depth)[None, :] >= depth - token_position[:, None]).astype(jnp.float32)
    state_is_valid = (token_position > 0).astype(jnp.float32)[:, None]
    position_indicator = (
        token_position[:, None] == jnp.arange(position_log_decay.shape[1])[None, :]
    ).astype(jnp.float32)
    head_first = lax.axis_index("tp") * heads_local
    stream = hidden
    states, values, writes, reads = ([], [], [], [])
    for layer_index in range(input_norm_gain.shape[0]):
        stream_float = stream.astype(jnp.float32)
        squares = jnp.sum(stream_float * stream_float, axis=1)
        normed = (stream_float * input_norm_gain[layer_index]).astype(jnp.bfloat16)
        pieces = [
            jnp.dot(normed, weight[layer_index], preferred_element_type=jnp.float32)
            for weight in (gate_matrix, input_matrix, write_matrix, read_matrix)
        ]
        step_term = jnp.dot(normed, step_matrix[layer_index], preferred_element_type=jnp.float32)
        heads_all = step_term.shape[1]
        width = sum(piece.shape[1] for piece in pieces)
        joined = jnp.concatenate(pieces + [step_term, squares[:, None]], axis=1)
        joined_mine = exchange_rows(joined, "dp", seq_local)
        mean_square = joined_mine[:, width + heads_all :] / D
        row_scale = lax.rsqrt(mean_square + epsilon)
        step_mine = joined_mine[:, width : width + heads_all]
        step_raw = lax.dynamic_slice_in_dim(step_mine, head_first, heads_local, 1) * row_scale
        scaled = joined_mine[:, :width] * row_scale
        proj_gate = scaled[:, :inner_local]
        value_row = scaled[:, inner_local : 2 * inner_local].astype(jnp.bfloat16)
        write_row = scaled[:, 2 * inner_local : 2 * inner_local + shared_local].astype(jnp.bfloat16)
        read_row = scaled[:, 2 * inner_local + shared_local :].astype(jnp.bfloat16)
        value_act, value_buf = convolve(
            history_input_rows[layer_index], value_row, input_filter_taps[layer_index], tap_valid
        )
        write_act, write_buf = convolve(
            history_write_rows[layer_index], write_row, write_filter_taps[layer_index], tap_valid
        )
        read_act, read_buf = convolve(
            history_read_rows[layer_index], read_row, read_filter_taps[layer_index], tap_valid
        )
        head_step_size = jax.nn.softplus(step_raw + step_size_bias[layer_index])
        current_log_decay = jnp.dot(
            position_indicator, position_log_decay[layer_index], precision=lax.Precision.HIGHEST
        )
        current_decay = (
            jnp.exp(-jnp.exp(log_decay_rate[layer_index]) * head_step_size + current_log_decay)
            * state_is_valid
        )
        value_heads = value_act.reshape(seq_local, heads_local, head_dim)
        write_heads = spread_groups(write_act, seq_local, groups_local, per_group, state_dim)
        read_heads = spread_groups(read_act, seq_local, groups_local, per_group, state_dim)
        updated = (
            current_decay[:, :, None, None] * recurrent_head_state[layer_index]
            + (head_step_size[:, :, None] * value_heads)[:, :, :, None] * write_heads[:, :, None, :]
        )
        readout = jnp.einsum("shpn,shn->shp", updated, read_heads, precision=lax.Precision.HIGHEST)
        mixed_heads = (
            readout + direct_path_gain[layer_index][None, :, None] * value_heads
        ) * jax.nn.silu(proj_gate.reshape(seq_local, heads_local, head_dim))
        grouped = mixed_heads.reshape(seq_local, groups_local, per_group * head_dim)
        grouped = grouped * lax.rsqrt(jnp.mean(grouped * grouped, axis=2, keepdims=True) + epsilon)
        gated_rows = (
            grouped.reshape(seq_local, inner_local) * grouped_norm_gain[layer_index]
        ).astype(jnp.bfloat16)
        out_weight = output_matrix[layer_index]

        gathered = gather_rows(gated_rows, "dp")
        partial_out = jnp.dot(gathered, out_weight, preferred_element_type=jnp.float32)
        branch = sum_copies(partial_out, "tp")
        stream = (stream_float + branch).astype(jnp.bfloat16)
        states.append(updated)
        values.append(value_buf)
        writes.append(write_buf)
        reads.append(read_buf)
    return (stream, jnp.stack(states), jnp.stack(values), jnp.stack(writes), jnp.stack(reads))


def solution(mesh):
    placed = (
        P("grp", "dp"),
        P(("grp", "dp")),
        P(None, "dp"),
        P(None, "dp", "tp"),
        P(None, "dp", "tp"),
        P(None, "dp", "tp"),
        P(None, "dp", "tp"),
        P(None, "dp", None),
        P(None, "tp"),
        P(None, "tp"),
        P(None, "tp"),
        P(None, None, "tp"),
        P(None, None, "tp"),
        P(None, None, "tp"),
        P(None, None, "tp"),
        P(None, "tp"),
        P(None, "tp", "dp"),
        P(None, ("grp", "dp"), "tp", None, None),
        P(None, ("grp", "dp"), None, "tp"),
        P(None, ("grp", "dp"), None, "tp"),
        P(None, ("grp", "dp"), None, "tp"),
    )
    return jax.shard_map(
        on_device,
        mesh=mesh,
        in_specs=placed,
        out_specs=(
            P("grp", "dp"),
            P(None, ("grp", "dp"), "tp", None, None),
            P(None, ("grp", "dp"), None, "tp"),
            P(None, ("grp", "dp"), None, "tp"),
            P(None, ("grp", "dp"), None, "tp"),
        ),
        check_vma=False,
    )
```

```python
import functools

import jax
import jax.numpy as jnp
from jax import lax
from jax.experimental import pallas as pl
from jax.experimental.pallas import tpu as pltpu
from jax.sharding import PartitionSpec as P

D = 2048


epsilon = 1e-06
LANES = 128
TABLE = 64
f32 = jnp.float32
bf16 = jnp.bfloat16
VMEM = pltpu.VMEM


def lane_iota(shape):
    return lax.broadcasted_iota(jnp.int32, shape, 1)


def pack(row):
    return jnp.concatenate(
        [row[:, i : i + LANES] for i in range(0, row.shape[1], LANES)], axis=0
    )


def unpack(rows):
    return jnp.concatenate([rows[i : i + 1] for i in range(rows.shape[0])], axis=1)


def column(row, count):
    wide = jnp.broadcast_to(row[:, :count], (count, count))
    eye = lane_iota((count, count)) == lax.broadcasted_iota(jnp.int32, (count, count), 0)
    return jnp.broadcast_to(
        jnp.sum(jnp.where(eye, wide, 0.0), axis=1, keepdims=True), (count, LANES)
    )


def interleave(scratch, rows):
    half = rows.shape[0] // 2
    scratch[...] = rows
    even = scratch[pl.ds(0, half, stride=2), :]
    odd = scratch[pl.ds(1, half, stride=2), :]
    return jnp.where(lane_iota((half, LANES)) < LANES // 2, even, odd)


def tree_sum(parts):
    while len(parts) > 1:
        parts = [parts[i] + parts[i + 1] for i in range(0, len(parts), 2)]
    return parts[0]


def start_all(pairs, sems):
    copies = [pltpu.make_async_copy(source, target, sems.at[i]) for i, (source, target) in enumerate(pairs)]
    for copy in copies:
        copy.start()
    return copies


def halves(source, target, count=2):
    size = target.shape[0] // count
    return [
        (source.at[pl.ds(i * size, size)], target.at[pl.ds(i * size, size)]) for i in range(count)
    ]


def project_rows(dims, x, gain, held, waits, outs, scratch):
    seqs, chunks, shared, heads, rows, fan = dims
    squares = jnp.sum(x * x, axis=1, keepdims=True)
    normed = (x * gain).astype(bf16)
    count = x.shape[0]
    base = 0
    for i in range(4):
        for copy in waits[i]:
            copy.wait()
        piece = jnp.dot(normed, held[i][...], preferred_element_type=f32)
        for c in range(piece.shape[1] // LANES):
            scratch[pl.ds((base + c) * count, count), :] = piece[:, c * LANES : (c + 1) * LANES]
        base += piece.shape[1] // LANES
    for copy in waits[4]:
        copy.wait()
    step = lax.dot_general(
        normed, held[4][...], (((1,), (1,)), ((), ())), preferred_element_type=f32
    )
    width = step.shape[1]
    if width < LANES:
        step = jnp.concatenate([step, jnp.zeros((count, LANES - width), f32)], axis=1)
    shift = lax.rem(LANES - lax.axis_index("tp") * heads, LANES)
    step = pltpu.roll(step, shift, 1)
    last = jnp.where(lane_iota((count, LANES)) < heads, step, jnp.broadcast_to(squares, (count, LANES)))
    scratch[pl.ds(base * count, count), :] = last
    for i in range(base + 1, rows):
        scratch[pl.ds(i * count, count), :] = jnp.zeros((count, LANES), f32)
    me = lax.axis_index("dp")
    for mask in range(fan):
        first = lax.bitwise_xor(me, jnp.int32(mask)) * seqs
        for s in range(seqs):
            outs[mask][pl.ds(s * rows, rows), :] = scratch[pl.ds(first + s, rows, stride=count), :]


def first_project_kernel(dims, layer, *refs):
    fan = dims[5]
    refs = list(refs)
    x_hbm, gain_hbm = refs[:2]
    weights = refs[2:7]
    outs = refs[7 : 7 + fan]
    x_ref, gain_ref = refs[7 + fan : 9 + fan]
    held = refs[9 + fan : 14 + fan]
    scratch, sems = refs[14 + fan :]
    pairs = [(x_hbm, x_ref), (gain_hbm, gain_ref)]
    spans = []
    for source, target in zip(weights, held):
        more = halves(source.at[layer], target)
        spans.append((len(pairs), len(pairs) + len(more)))
        pairs += more
    copies = start_all(pairs, sems)
    copies[0].wait()
    copies[1].wait()
    waits = [copies[low:high] for low, high in spans]
    project_rows(
        dims, x_ref[...].astype(f32), gain_ref[layer : layer + 1, :], held, waits, outs, scratch
    )


def next_project_kernel(dims, layer, *refs):
    fan, tp = dims[5], lax.axis_size("tp")
    refs = list(refs)
    x_ref, parts, gain_ref = refs[0], refs[1 : 1 + tp], refs[1 + tp]
    held = refs[2 + tp : 7 + tp]
    new_ref = refs[7 + tp]
    outs = refs[8 + tp : 8 + tp + fan]
    scratch = refs[-1]
    new = (x_ref[...].astype(f32) + tree_sum([part[...] for part in parts])).astype(bf16)
    new_ref[...] = new
    project_rows(
        dims, new.astype(f32), gain_ref[layer : layer + 1, :], held, [[]] * 5, outs, scratch
    )


def table_kernel(dims, *refs):
    seqs, chunks, shared, heads, rows, fan = dims
    lengths_ref = refs[0]
    sources = refs[2:13]
    state, weight, gain, hidden = refs[13:17]
    out, state_out, weight_out, gain_out, hidden_out, split_out = refs[17:23]
    hv, hw, hr, tv, tw, tr, bias, rate, direct, pos, norm = held = refs[23:34]
    scratch, sems = refs[34:]
    copies = start_all(
        list(zip(sources, held))
        + [(gain, gain_out), (hidden, hidden_out), (state.at[0], state_out), (weight.at[0], weight_out)],
        sems,
    )
    for copy in copies[: len(held)]:
        copy.wait()
    layers, depth = hv.shape[:2]
    for layer in range(layers):
        taps = [ref[layer].astype(f32) for ref in (tv, tw, tr)]
        out[layer, 0:chunks] = pack(taps[0][depth : depth + 1])
        out[layer, chunks : 2 * chunks] = jnp.concatenate(
            [pack(taps[1][depth : depth + 1]), pack(taps[2][depth : depth + 1])], axis=0
        )
        out[layer, 2 * chunks : 3 * chunks] = interleave(
            scratch, column(direct[layer : layer + 1, :], heads)
        )
        out[layer, 3 * chunks : 4 * chunks] = pack(norm[layer : layer + 1, :])
        at = 4 * chunks
        out[layer, at : at + heads] = column(bias[layer : layer + 1, :], heads)
        at += heads
        out[layer, at : at + heads] = -jnp.exp(column(rate[layer : layer + 1, :], heads))
        at += heads
        for s in range(seqs):
            position = lengths_ref[s] - 1
            sums = []
            for ref, tap in zip((hv, hw, hr), taps):
                total = None
                for k in range(depth):
                    term = ref[layer, k].astype(f32)[s : s + 1] * tap[k : k + 1]
                    term = jnp.where(depth - position <= k, term, 0.0)
                    total = term if total is None else total + term
                sums.append(pack(total))
            out[layer, at : at + chunks] = sums[0]
            at += chunks
            out[layer, at : at + chunks] = jnp.concatenate(sums[1:], axis=0)
            at += chunks
            logs = pos[layer]
            here = jnp.sum(jnp.where(lane_iota(logs.shape) == position, logs, 0.0), axis=1, keepdims=True)
            out[layer, at : at + heads] = jnp.where(
                position > 0, jnp.broadcast_to(here, (heads, LANES)), -1e30
            )
            at += heads
    for copy in copies[len(held) : -1]:
        copy.wait()
    split_state(state_out, split_out)
    copies[-1].wait()


def two_terms(x):
    high = x.astype(bf16)
    return high, (x - high.astype(f32)).astype(bf16)


def split_state(held, out):
    seqs, heads, depth, _ = held.shape
    for s in range(seqs):
        for h in range(heads):
            high, rest = two_terms(held[s, h])
            at = (s * heads + h) * depth
            out[at : at + depth, 0:LANES] = high
            out[at : at + depth, LANES : 2 * LANES] = rest


def fetch_state_kernel(layer, *refs):
    state, weight, held, weight_out, split_out, sems = refs[1:]
    copies = start_all(halves(state.at[layer], held) + halves(weight.at[layer], weight_out), sems)
    copies[0].wait()
    copies[1].wait()
    split_state(held, split_out)
    copies[2].wait()
    copies[3].wait()


def fetch_kernel(plan, *refs):
    count = len(plan)
    sources, targets, sems = refs[1 : 1 + count], refs[1 + count : 1 + 2 * count], refs[-1]
    pairs = []
    for block, source, target in zip(plan, sources, targets):
        pairs += halves(source if block is None else source.at[block], target)
    for copy in start_all(pairs, sems):
        copy.wait()


def update_kernel(dims, layer, *refs):
    seqs, chunks, shared, heads, rows, fan = dims
    lead_ref, acts, decays, held = refs[:4]
    out, made, sems = refs[-3:]
    per_group = heads // shared
    half = LANES // 2
    lead = lead_ref[...]
    count = lead.shape[0]
    high, rest = two_terms(lead)
    last = lead - high.astype(f32) - rest.astype(f32)
    terms = [high.astype(f32)] * 3 + [rest.astype(f32)] * 2 + [last]
    blank = jnp.zeros((LANES - 6 * count, LANES), f32)
    left = jnp.transpose(jnp.concatenate(terms + [blank], axis=0)).astype(bf16)
    at_row = lax.broadcasted_iota(jnp.int32, (count, LANES), 0)
    copies = []
    for s in range(seqs):
        for g in range(shared):
            write = acts[s, g : g + 1, :]
            high, rest = two_terms(write)
            last = write - high.astype(f32) - rest.astype(f32)
            high, rest = high.astype(f32), rest.astype(f32)
            right = []
            for i in range(per_group // 2):
                here = at_row == s * chunks + g * per_group // 2 + i
                terms = [jnp.where(here, jnp.broadcast_to(t, (count, LANES)), 0.0) for t in (high, rest, last)]
                order = [terms[0], terms[1], terms[2], terms[0], terms[1], terms[0], blank]
                right.append(jnp.concatenate(order, axis=0).astype(bf16))
            added = jnp.dot(left, jnp.concatenate(right, axis=1), preferred_element_type=f32)
            for i in range(per_group // 2):
                for j in range(2):
                    h = g * per_group + 2 * i + j
                    made[s, h] = (
                        decays[s, h : h + 1, :] * held[s, h]
                        + added[j * half : (j + 1) * half, i * LANES : (i + 1) * LANES]
                    )
            copy = pltpu.make_async_copy(
                made.at[s, pl.ds(g * per_group, per_group)],
                out.at[layer, s, pl.ds(g * per_group, per_group)],
                sems.at[s * shared + g],
            )
            copy.start()
            copies.append(copy)
    for copy in copies:
        copy.wait()


def silu(x):
    return x / (1.0 + jnp.exp(-x))


def mix_kernel(dims, layer, *refs):
    seqs, chunks, shared, heads, rows, fan = dims
    parts, table, split = refs[:fan], refs[fan], refs[fan + 1]
    gated_ref, rows_ref, lead_ref, acts, decays, pairs = refs[fan + 2 :]
    groups = shared
    per_group = heads // groups
    span = per_group // 2
    total = tree_sum([part[...] for part in parts])
    at_row = lax.broadcasted_iota(jnp.int32, (chunks, LANES), 0)
    for s in range(seqs):
        block = total[s * rows : (s + 1) * rows]
        at = 4 * chunks + 2 * heads + s * (2 * chunks + heads)
        last = block[2 * chunks + 2 * shared : 2 * chunks + 2 * shared + 1]
        scale = lax.rsqrt(last[:, LANES // 2 : LANES // 2 + 1] / D + epsilon)
        share_row = (block[2 * chunks : 2 * chunks + 2 * shared] * scale).astype(bf16).astype(f32)
        act = silu(
            share_row * table[layer, chunks : 2 * chunks]
            + table[layer, at + chunks : at + chunks + 2 * shared]
        )
        acts[s] = act
        sums = jnp.zeros((chunks, LANES), f32)
        write_rows, read_rows = [], []
        for g in range(groups):
            read = act[groups + g : groups + g + 1]
            here = (at_row >= g * span) & (at_row < (g + 1) * span)
            high, rest = two_terms(jnp.where(here, jnp.broadcast_to(read, (chunks, LANES)), 0.0))
            left = jnp.concatenate([high.astype(f32), rest.astype(f32)], axis=0).astype(bf16)
            size = span * LANES
            first = (s * groups + g) * size
            product = lax.dot_general(
                jnp.concatenate([left, left], axis=1),
                split[first : first + size, :],
                (((1,), (1,)), ((), ())),
                preferred_element_type=f32,
            )
            product = product[0:chunks] + product[chunks : 2 * chunks]
            for i in range(span):
                sums = jnp.where(at_row == g * span + i, product[:, i * LANES : (i + 1) * LANES], sums)
            write_rows += [act[g : g + 1]] * span
            read_rows += [read] * span
        overlap = jnp.sum(
            jnp.concatenate(write_rows, axis=0) * jnp.concatenate(read_rows, axis=0), axis=1, keepdims=True
        )
        gate = silu(block[0:chunks] * scale)
        value_row = (block[chunks : 2 * chunks] * scale).astype(bf16).astype(f32)
        rows_ref[s, 0:chunks] = value_row
        rows_ref[s, chunks : chunks + 2 * shared] = share_row
        value_act = silu(value_row * table[layer, 0:chunks] + table[layer, at : at + chunks])
        raw = column(last * scale, heads) + table[layer, 4 * chunks : 4 * chunks + heads]
        step = jnp.maximum(raw, 0.0) + jnp.log1p(jnp.exp(-jnp.abs(raw)))
        decay = jnp.exp(
            table[layer, 4 * chunks + heads : 4 * chunks + 2 * heads] * step
            + table[layer, at + 2 * chunks : at + 2 * chunks + heads]
        )
        decays[s] = decay
        lead = interleave(pairs.at[2 * s], step) * value_act
        lead_ref[s * chunks : (s + 1) * chunks, :] = lead
        readout = interleave(pairs.at[2 * s + 1], decay) * sums + lead * overlap
        mixed = (readout + table[layer, 2 * chunks : 3 * chunks] * value_act) * gate
        power = jnp.broadcast_to(jnp.sum(mixed * mixed, axis=1, keepdims=True), (chunks, LANES))
        other = jnp.where(
            lax.rem(at_row, 2) == 0, pltpu.roll(power, chunks - 1, 0), pltpu.roll(power, 1, 0)
        )
        mixed = mixed * lax.rsqrt((power + other) / (2 * LANES) + epsilon)
        gated_ref[s * chunks : (s + 1) * chunks, :] = (
            mixed * table[layer, 3 * chunks : 4 * chunks]
        ).astype(bf16)


def output_kernel(dims, *refs):
    seqs, chunks, shared, heads, rows, fan = dims
    parts, weight = refs[:fan], refs[fan]
    out, scratch = refs[fan + 2 :]
    me = lax.axis_index("dp")
    block = seqs * chunks
    for mask in range(fan):
        start = pl.multiple_of(lax.bitwise_xor(me, jnp.int32(mask)) * block, block)
        scratch[pl.ds(start, block), :] = parts[mask][...].astype(f32)
    whole = jnp.concatenate(
        [scratch[pl.ds(c, fan * seqs, stride=chunks), :] for c in range(chunks)], axis=1
    ).astype(bf16)
    out[...] = jnp.dot(whole, weight[...], preferred_element_type=f32)


def close_kernel(x_ref, *refs):
    out = refs[-1]
    out[...] = (x_ref[...].astype(f32) + tree_sum([ref[...] for ref in refs[:-1]])).astype(bf16)


def buffer_kernel(dims, layers, *refs):
    seqs, chunks, shared, heads, rows, fan = dims
    new_rows = refs[1 : 1 + layers]
    past = refs[1 + layers : 4 + layers]
    outs = refs[4 + layers : 7 + layers]
    held = refs[7 + layers : 10 + layers]
    built = refs[10 + layers : 13 + layers]
    sems = refs[-1]
    for copy in start_all(list(zip(past, held)), sems):
        copy.wait()
    spans = ((0, chunks), (chunks, chunks + shared), (chunks + shared, chunks + 2 * shared))
    for old, new, (low, high) in zip(held, built, spans):
        depth = old.shape[1]
        for layer in range(layers):
            for k in range(depth - 1):
                new[layer, k] = old[layer, k + 1]
            new[layer, depth - 1] = jnp.concatenate(
                [unpack(new_rows[layer][s, low:high]) for s in range(seqs)], axis=0
            ).astype(bf16)
    for copy in start_all(list(zip(built, outs)), sems):
        copy.wait()


def full(memory=VMEM):
    return pl.BlockSpec(memory_space=memory)


HBM = pltpu.HBM


def place(arrays, memory):
    return [pltpu.with_memory_space_constraint(array, memory) for array in arrays]


def cost(flops, moved):
    return pl.CostEstimate(flops=flops, bytes_accessed=moved, transcendentals=0)


def direct(axis):
    size = lax.axis_size(axis)
    return size <= 8 and size & (size - 1) == 0


def swap(array, axis, mask):
    return lax.ppermute(array, axis, [(i, i ^ mask) for i in range(lax.axis_size(axis))])


def swaps(array, axis):
    return [array] + [swap(array, axis, mask) for mask in range(1, lax.axis_size(axis))]


def on_device_kernels(
    hidden,
    lengths,
    input_norm_gain,
    gate_matrix,
    input_matrix,
    write_matrix,
    read_matrix,
    step_matrix,
    step_size_bias,
    log_decay_rate,
    direct_path_gain,
    input_filter_taps,
    write_filter_taps,
    read_filter_taps,
    position_log_decay,
    grouped_norm_gain,
    output_matrix,
    recurrent_head_state,
    history_input_rows,
    history_write_rows,
    history_read_rows,
):
    layers, seqs, heads = recurrent_head_state.shape[:3]
    chunks = input_filter_taps.shape[2] // LANES
    shared = write_filter_taps.shape[2] // LANES
    rows = -(-(2 * chunks + 2 * shared + 1) // 8) * 8
    fan = lax.axis_size("dp")
    dims = (seqs, chunks, shared, heads, rows, fan)
    count = hidden.shape[0]
    weights = (
        gate_matrix,
        input_matrix,
        write_matrix,
        read_matrix,
        jnp.swapaxes(step_matrix, 1, 2),
    )
    past = [
        jnp.swapaxes(h, 1, 2) for h in (history_input_rows, history_write_rows, history_read_rows)
    ]
    state = recurrent_head_state
    params = pltpu.CompilerParams(vmem_limit_bytes=12 * 1024 * 1024)
    table_rows = 4 * chunks + 2 * heads + seqs * (2 * chunks + heads)
    message = pltpu.VMEM((seqs * rows, LANES), f32)
    pool = pltpu.VMEM((rows * count, LANES), f32)

    def fetch(after, blocks, name):
        sources = [array for array, _ in blocks]
        plan = [block for _, block in blocks]
        return pl.pallas_call(
            functools.partial(fetch_kernel, plan),
            out_shape=[
                pltpu.VMEM(a.shape if block is None else a.shape[1:], a.dtype) for a, block in blocks
            ],
            in_specs=[full()] + [full(HBM)] * len(blocks),
            out_specs=[full()] * len(blocks),
            scratch_shapes=[pltpu.SemaphoreType.DMA((2 * len(blocks),))],
            compiler_params=params,
            cost_estimate=cost(4_000_000, 1_000_000),
            name=name,
        )(*place([after], VMEM), *place(sources, HBM))

    def fetch_state(layer, after):
        return pl.pallas_call(
            functools.partial(fetch_state_kernel, layer),
            out_shape=[
                pltpu.VMEM(state.shape[1:], f32),
                pltpu.VMEM(output_matrix.shape[1:], bf16),
                pltpu.VMEM((seqs * heads * state.shape[3], 2 * LANES), bf16),
            ],
            in_specs=[full()] + [full(HBM)] * 2,
            out_specs=[full()] * 3,
            scratch_shapes=[pltpu.SemaphoreType.DMA((4,))],
            compiler_params=params,
            cost_estimate=cost(4_000_000, 1_000_000),
            name="fetch",
        )(*place([after], VMEM), *place([state, output_matrix], HBM))

    def mix(layer, parts, tables, split):
        return pl.pallas_call(
            functools.partial(mix_kernel, dims, layer),
            out_shape=[
                pltpu.VMEM((seqs * chunks, LANES), bf16),
                pltpu.VMEM((seqs, chunks + 2 * shared, LANES), f32),
                pltpu.VMEM((seqs * chunks, LANES), f32),
                pltpu.VMEM((seqs, 2 * shared, LANES), f32),
                pltpu.VMEM((seqs, heads, LANES), f32),
            ],
            in_specs=[full()] * (fan + 2),
            out_specs=[full()] * 5,
            scratch_shapes=[pltpu.VMEM((2 * seqs, heads, LANES), f32)],
            compiler_params=params,
            name="mix",
        )(*place(list(parts) + [tables, split], VMEM))

    def update(layer, factors, held, states):
        given = place([*factors, held], VMEM)
        if states is not None:
            given += place([states], HBM)
        return pl.pallas_call(
            functools.partial(update_kernel, dims, layer),
            out_shape=jax.ShapeDtypeStruct(state.shape, f32),
            in_specs=[full()] * 4 + [full(HBM)] * (len(given) - 4),
            out_specs=full(HBM),
            scratch_shapes=[
                pltpu.VMEM(state.shape[1:], f32),
                pltpu.SemaphoreType.DMA((seqs * shared,)),
            ],
            input_output_aliases={4: 0} if states is not None else {},
            compiler_params=params,
            cost_estimate=cost(4_000_000, 1_000_000),
            name="update",
        )(*given)

    def output(parts, weight, states):
        return pl.pallas_call(
            functools.partial(output_kernel, dims),
            out_shape=pltpu.VMEM((count, output_matrix.shape[2]), f32),
            in_specs=[full()] * (fan + 1) + [full(HBM)],
            out_specs=full(),
            scratch_shapes=[pltpu.VMEM((fan * seqs * chunks, LANES), f32)],
            compiler_params=params,
            name="output",
        )(*place(list(parts) + [weight], VMEM), *place([states], HBM))

    given = [hidden, input_norm_gain, *weights]
    made = pl.pallas_call(
        functools.partial(first_project_kernel, dims, 0),
        out_shape=[message] * fan,
        in_specs=[full(HBM) for _ in given],
        out_specs=[full()] * fan,
        scratch_shapes=[pltpu.VMEM(hidden.shape, bf16), pltpu.VMEM(input_norm_gain.shape, f32)]
        + [pltpu.VMEM(w.shape[1:], bf16) for w in weights]
        + [pool, pltpu.SemaphoreType.DMA((12,))],
        compiler_params=params,
        name="project",
    )(*place(given, HBM))
    small = past + [
        input_filter_taps,
        write_filter_taps,
        read_filter_taps,
        step_size_bias,
        log_decay_rate,
        direct_path_gain,
        jnp.swapaxes(position_log_decay, 1, 2),
        grouped_norm_gain,
    ]
    tables, held, weight, gain, stream, split = pl.pallas_call(
        functools.partial(table_kernel, dims),
        out_shape=[
            pltpu.VMEM((layers, table_rows, LANES), f32),
            pltpu.VMEM(state.shape[1:], f32),
            pltpu.VMEM(output_matrix.shape[1:], bf16),
            pltpu.VMEM(input_norm_gain.shape, f32),
            pltpu.VMEM(hidden.shape, bf16),
            pltpu.VMEM((seqs * heads * state.shape[3], 2 * LANES), bf16),
        ],
        in_specs=[full(pltpu.SMEM), full()] + [full(HBM)] * (len(small) + 4),
        out_specs=[full()] * 6,
        scratch_shapes=[pltpu.VMEM(a.shape, a.dtype) for a in small]
        + [pltpu.VMEM((heads, LANES), f32), pltpu.SemaphoreType.DMA((len(small) + 4,))],
        compiler_params=params,
        cost_estimate=cost(4_000_000, 1_000_000),
        name="tables",
    )(
        lengths,
        *place([made[0]], VMEM),
        *place(small + [state, output_matrix, input_norm_gain, hidden], HBM),
    )
    states = None
    new_rows = []
    for layer in range(layers):
        parts = [made[0]] + [swap(made[mask], "dp", mask) for mask in range(1, fan)]
        if layer > 0:
            held, weight, split = fetch_state(layer, made[0])
        gated, row_values, *factors = mix(layer, parts, tables, split)
        new_rows.append(row_values)
        parts = swaps(gated, "dp")
        states = update(layer, factors, held, states)
        own = output(parts, weight, states)
        partial = swaps(own, "tp")
        if layer + 1 < layers:
            ahead = fetch(own, [(w, layer + 1) for w in weights], "fetch")
            stream, *made = pl.pallas_call(
                functools.partial(next_project_kernel, dims, layer + 1),
                out_shape=[pltpu.VMEM(hidden.shape, bf16)] + [message] * fan,
                in_specs=[full()] * (2 + len(partial) + len(weights)),
                out_specs=[full()] * (1 + fan),
                scratch_shapes=[pool],
                compiler_params=params,
                name="project",
            )(*place([stream, *partial, gain, *ahead], VMEM))
    buffers = pl.pallas_call(
        functools.partial(buffer_kernel, dims, layers),
        out_shape=[jax.ShapeDtypeStruct(h.shape, bf16) for h in past],
        in_specs=[full()] * (1 + layers) + [full(HBM)] * 3,
        out_specs=[full(HBM)] * 3,
        scratch_shapes=[pltpu.VMEM(h.shape, bf16) for h in past] * 2 + [pltpu.SemaphoreType.DMA((3,))],
        compiler_params=params,
        cost_estimate=cost(4_000_000, 1_000_000),
        name="buffers",
    )(*place([own] + new_rows, VMEM), *place(past, HBM))
    buffers = [jnp.swapaxes(b, 1, 2) for b in buffers]
    stream = pl.pallas_call(
        close_kernel,
        out_shape=jax.ShapeDtypeStruct(hidden.shape, bf16),
        in_specs=[full()] * (1 + len(partial)),
        out_specs=full(),
        compiler_params=params,
        name="close",
    )(*place([stream, *partial], VMEM))
    return (stream, states, *buffers)


def kernels_fit(state, taps, write_taps, hidden, output_matrix, step_matrix):
    layers, seqs, heads, head_dim, state_dim = state.shape
    shared = write_taps.shape[2] // LANES
    chunks = taps.shape[2] // LANES
    return (
        direct("dp")
        and direct("tp")
        and state_dim == LANES
        and head_dim * 2 == LANES
        and shared > 0
        and heads == 4 * shared
        and chunks == 2 * shared
        and chunks % 8 == 0
        and heads % 16 == 0
        and seqs * chunks <= LANES
        and seqs * chunks % 16 == 0
        and hidden.shape[0] == seqs * lax.axis_size("dp")
        and hidden.shape[0] % 8 == 0
        and hidden.shape[1] % LANES == 0
        and output_matrix.shape[2] % LANES == 0
        and step_matrix.shape[2] <= LANES
        and heads <= LANES // 2
    )


def convolve(buffer, new_row, weights, tap_valid):
    tap_rows = weights.astype(jnp.float32)
    depth = weights.shape[0] - 1
    summed = new_row.astype(jnp.float32) * tap_rows[depth]
    for k in range(depth):
        summed = summed + buffer[:, k].astype(jnp.float32) * tap_rows[k] * tap_valid[:, k : k + 1]
    shifted = jnp.concatenate([buffer[:, 1:], new_row[:, None]], axis=1)
    return (jax.nn.silu(summed), shifted)


def spread_groups(rows, seq_local, groups_local, per_group, state_dim):
    grouped = rows.reshape(seq_local, groups_local, 1, state_dim)
    return jnp.broadcast_to(grouped, (seq_local, groups_local, per_group, state_dim)).reshape(
        seq_local, groups_local * per_group, state_dim
    )


def exchange_rows(rows, axis, count):
    if not direct(axis):
        return lax.psum_scatter(rows, axis, scatter_dimension=0, tiled=True)
    me = lax.axis_index(axis)
    parts = [
        lax.dynamic_slice_in_dim(rows, (me ^ mask) * count, count, 0)
        for mask in range(lax.axis_size(axis))
    ]
    return tree_sum([parts[0]] + [swap(parts[mask], axis, mask) for mask in range(1, len(parts))])


def gather_rows(rows, axis):
    if not direct(axis):
        return lax.all_gather(rows, axis, axis=0, tiled=True)
    me, size = lax.axis_index(axis), lax.axis_size(axis)
    parts = [rows] + [swap(rows, axis, mask) for mask in range(1, size)]
    whole = jnp.zeros((size,) + rows.shape, rows.dtype)
    for mask in range(size):
        whole = lax.dynamic_update_index_in_dim(whole, parts[mask], me ^ mask, 0)
    return whole.reshape((size * rows.shape[0],) + rows.shape[1:])


def sum_copies(rows, axis):
    if not direct(axis):
        return lax.psum(rows, axis)
    return tree_sum([rows] + [swap(rows, axis, mask) for mask in range(1, lax.axis_size(axis))])


def on_device_plain(
    hidden,
    lengths,
    input_norm_gain,
    gate_matrix,
    input_matrix,
    write_matrix,
    read_matrix,
    step_matrix,
    step_size_bias,
    log_decay_rate,
    direct_path_gain,
    input_filter_taps,
    write_filter_taps,
    read_filter_taps,
    position_log_decay,
    grouped_norm_gain,
    output_matrix,
    recurrent_head_state,
    history_input_rows,
    history_write_rows,
    history_read_rows,
):
    seq_local = lengths.shape[0]
    heads_local = step_size_bias.shape[1]
    head_dim = recurrent_head_state.shape[3]
    state_dim = recurrent_head_state.shape[4]
    groups_local = write_filter_taps.shape[2] // state_dim
    per_group = heads_local // groups_local
    inner_local = heads_local * head_dim
    shared_local = groups_local * state_dim
    depth = input_filter_taps.shape[1] - 1
    token_position = lengths - 1
    tap_valid = (jnp.arange(depth)[None, :] >= depth - token_position[:, None]).astype(jnp.float32)
    state_is_valid = (token_position > 0).astype(jnp.float32)[:, None]
    position_indicator = (
        token_position[:, None] == jnp.arange(position_log_decay.shape[1])[None, :]
    ).astype(jnp.float32)
    head_first = lax.axis_index("tp") * heads_local
    stream = hidden
    states, values, writes, reads = ([], [], [], [])
    for layer_index in range(input_norm_gain.shape[0]):
        stream_float = stream.astype(jnp.float32)
        squares = jnp.sum(stream_float * stream_float, axis=1)
        normed = (stream_float * input_norm_gain[layer_index]).astype(jnp.bfloat16)
        pieces = [
            jnp.dot(normed, weight[layer_index], preferred_element_type=jnp.float32)
            for weight in (gate_matrix, input_matrix, write_matrix, read_matrix)
        ]
        step_term = jnp.dot(normed, step_matrix[layer_index], preferred_element_type=jnp.float32)
        heads_all = step_term.shape[1]
        width = sum(piece.shape[1] for piece in pieces)
        joined = jnp.concatenate(pieces + [step_term, squares[:, None]], axis=1)
        joined_mine = exchange_rows(joined, "dp", seq_local)
        mean_square = joined_mine[:, width + heads_all :] / D
        row_scale = lax.rsqrt(mean_square + epsilon)
        step_mine = joined_mine[:, width : width + heads_all]
        step_raw = lax.dynamic_slice_in_dim(step_mine, head_first, heads_local, 1) * row_scale
        scaled = joined_mine[:, :width] * row_scale
        proj_gate = scaled[:, :inner_local]
        value_row = scaled[:, inner_local : 2 * inner_local].astype(jnp.bfloat16)
        write_row = scaled[:, 2 * inner_local : 2 * inner_local + shared_local].astype(jnp.bfloat16)
        read_row = scaled[:, 2 * inner_local + shared_local :].astype(jnp.bfloat16)
        value_act, value_buf = convolve(
            history_input_rows[layer_index], value_row, input_filter_taps[layer_index], tap_valid
        )
        write_act, write_buf = convolve(
            history_write_rows[layer_index], write_row, write_filter_taps[layer_index], tap_valid
        )
        read_act, read_buf = convolve(
            history_read_rows[layer_index], read_row, read_filter_taps[layer_index], tap_valid
        )
        head_step_size = jax.nn.softplus(step_raw + step_size_bias[layer_index])
        current_log_decay = jnp.dot(
            position_indicator, position_log_decay[layer_index], precision=lax.Precision.HIGHEST
        )
        current_decay = (
            jnp.exp(-jnp.exp(log_decay_rate[layer_index]) * head_step_size + current_log_decay)
            * state_is_valid
        )
        value_heads = value_act.reshape(seq_local, heads_local, head_dim)
        write_heads = spread_groups(write_act, seq_local, groups_local, per_group, state_dim)
        read_heads = spread_groups(read_act, seq_local, groups_local, per_group, state_dim)
        updated = (
            current_decay[:, :, None, None] * recurrent_head_state[layer_index]
            + (head_step_size[:, :, None] * value_heads)[:, :, :, None] * write_heads[:, :, None, :]
        )
        readout = jnp.einsum("shpn,shn->shp", updated, read_heads, precision=lax.Precision.HIGHEST)
        mixed_heads = (
            readout + direct_path_gain[layer_index][None, :, None] * value_heads
        ) * jax.nn.silu(proj_gate.reshape(seq_local, heads_local, head_dim))
        grouped = mixed_heads.reshape(seq_local, groups_local, per_group * head_dim)
        grouped = grouped * lax.rsqrt(jnp.mean(grouped * grouped, axis=2, keepdims=True) + epsilon)
        gated_rows = (
            grouped.reshape(seq_local, inner_local) * grouped_norm_gain[layer_index]
        ).astype(jnp.bfloat16)
        out_weight = output_matrix[layer_index]

        gathered = gather_rows(gated_rows, "dp")
        partial_out = jnp.dot(gathered, out_weight, preferred_element_type=jnp.float32)
        branch = sum_copies(partial_out, "tp")
        stream = (stream_float + branch).astype(jnp.bfloat16)
        states.append(updated)
        values.append(value_buf)
        writes.append(write_buf)
        reads.append(read_buf)
    return (stream, jnp.stack(states), jnp.stack(values), jnp.stack(writes), jnp.stack(reads))


def on_device(*args):
    hidden, taps, write_taps = args[0], args[11], args[12]
    if kernels_fit(args[17], taps, write_taps, hidden, args[16], args[7]):
        return on_device_kernels(*args)
    return on_device_plain(*args)


def solution(mesh):
    placed = (
        P("grp", "dp"),
        P(("grp", "dp")),
        P(None, "dp"),
        P(None, "dp", "tp"),
        P(None, "dp", "tp"),
        P(None, "dp", "tp"),
        P(None, "dp", "tp"),
        P(None, "dp", None),
        P(None, "tp"),
        P(None, "tp"),
        P(None, "tp"),
        P(None, None, "tp"),
        P(None, None, "tp"),
        P(None, None, "tp"),
        P(None, None, "tp"),
        P(None, "tp"),
        P(None, "tp", "dp"),
        P(None, ("grp", "dp"), "tp", None, None),
        P(None, ("grp", "dp"), None, "tp"),
        P(None, ("grp", "dp"), None, "tp"),
        P(None, ("grp", "dp"), None, "tp"),
    )
    return jax.shard_map(
        on_device,
        mesh=mesh,
        in_specs=placed,
        out_specs=(
            P("grp", "dp"),
            P(None, ("grp", "dp"), "tp", None, None),
            P(None, ("grp", "dp"), None, "tp"),
            P(None, ("grp", "dp"), None, "tp"),
            P(None, ("grp", "dp"), None, "tp"),
        ),
        check_vma=False,
    )
```

```python
import functools

import jax
import jax.numpy as jnp
from jax import lax
from jax.experimental import pallas as pl
from jax.experimental.pallas import tpu as pltpu
from jax.sharding import PartitionSpec as P


D = 2048


epsilon = 1e-06
LANES = 128
f32 = jnp.float32
bf16 = jnp.bfloat16
VMEM = pltpu.VMEM


def lane_iota(shape):
    return lax.broadcasted_iota(jnp.int32, shape, 1)


def pack(row):
    return jnp.concatenate(
        [row[:, i : i + LANES] for i in range(0, row.shape[1], LANES)], axis=0
    )


def unpack(rows):
    return jnp.concatenate([rows[i : i + 1] for i in range(rows.shape[0])], axis=1)


def column(row, count):
    wide = jnp.broadcast_to(row[:, :count], (count, count))
    eye = lane_iota((count, count)) == lax.broadcasted_iota(jnp.int32, (count, count), 0)
    return jnp.broadcast_to(
        jnp.sum(jnp.where(eye, wide, 0.0), axis=1, keepdims=True), (count, LANES)
    )


def interleave(scratch, rows):
    half = rows.shape[0] // 2
    scratch[...] = rows
    even = scratch[pl.ds(0, half, stride=2), :]
    odd = scratch[pl.ds(1, half, stride=2), :]
    return jnp.where(lane_iota((half, LANES)) < LANES // 2, even, odd)


def tree_sum(parts):
    while len(parts) > 1:
        parts = [parts[i] + parts[i + 1] for i in range(0, len(parts), 2)]
    return parts[0]


def start_all(pairs, sems):
    copies = [pltpu.make_async_copy(source, target, sems.at[i]) for i, (source, target) in enumerate(pairs)]
    for copy in copies:
        copy.start()
    return copies


def halves(source, target, count=2):
    size = target.shape[0] // count
    return [
        (source.at[pl.ds(i * size, size)], target.at[pl.ds(i * size, size)]) for i in range(count)
    ]


def project_rows(dims, x, gain, held, waits, outs, scratch):
    seqs, _, _, heads, rows, fan = dims
    squares = jnp.sum(x * x, axis=1, keepdims=True)
    normed = (x * gain).astype(bf16)
    count = x.shape[0]
    base = 0
    for i in range(4):
        for copy in waits[i]:
            copy.wait()
        piece = jnp.dot(normed, held[i][...], preferred_element_type=f32)
        for c in range(piece.shape[1] // LANES):
            scratch[pl.ds((base + c) * count, count), :] = piece[:, c * LANES : (c + 1) * LANES]
        base += piece.shape[1] // LANES
    for copy in waits[4]:
        copy.wait()
    step = lax.dot_general(
        normed, held[4][...], (((1,), (1,)), ((), ())), preferred_element_type=f32
    )
    width = step.shape[1]
    if width < LANES:
        step = jnp.concatenate([step, jnp.zeros((count, LANES - width), f32)], axis=1)
    shift = lax.rem(LANES - lax.axis_index("tp") * heads, LANES)
    step = pltpu.roll(step, shift, 1)
    last = jnp.where(lane_iota((count, LANES)) < heads, step, jnp.broadcast_to(squares, (count, LANES)))
    scratch[pl.ds(base * count, count), :] = last
    for i in range(base + 1, rows):
        scratch[pl.ds(i * count, count), :] = jnp.zeros((count, LANES), f32)
    me = lax.axis_index("dp")
    for mask in range(fan):
        first = lax.bitwise_xor(me, jnp.int32(mask)) * seqs
        for s in range(seqs):
            outs[mask][pl.ds(s * rows, rows), :] = scratch[pl.ds(first + s, rows, stride=count), :]


def first_project_kernel(dims, layer, *refs):
    fan = dims[5]
    refs = list(refs)
    x_hbm, gain_hbm = refs[:2]
    weights = refs[2:7]
    outs = refs[7 : 7 + fan]
    x_ref, gain_ref = refs[7 + fan : 9 + fan]
    held = refs[9 + fan : 14 + fan]
    scratch, sems = refs[14 + fan :]
    pairs = [(x_hbm, x_ref), (gain_hbm, gain_ref)]
    spans = []
    for source, target in zip(weights, held):
        more = halves(source.at[layer], target)
        spans.append((len(pairs), len(pairs) + len(more)))
        pairs += more
    copies = start_all(pairs, sems)
    copies[0].wait()
    copies[1].wait()
    waits = [copies[low:high] for low, high in spans]
    project_rows(
        dims, x_ref[...].astype(f32), gain_ref[layer : layer + 1, :], held, waits, outs, scratch
    )


def next_project_kernel(dims, layer, *refs):
    fan, tp = dims[5], lax.axis_size("tp")
    refs = list(refs)
    x_ref, parts, gain_ref = refs[0], refs[1 : 1 + tp], refs[1 + tp]
    held = refs[2 + tp : 7 + tp]
    new_ref = refs[7 + tp]
    outs = refs[8 + tp : 8 + tp + fan]
    scratch = refs[-1]
    new = (x_ref[...].astype(f32) + tree_sum([part[...] for part in parts])).astype(bf16)
    new_ref[...] = new
    project_rows(
        dims, new.astype(f32), gain_ref[layer : layer + 1, :], held, [[]] * 5, outs, scratch
    )


def table_kernel(dims, *refs):
    seqs, chunks, _, heads, _, _ = dims
    lengths_ref = refs[0]
    sources = refs[2:13]
    state, weight, gain, hidden = refs[13:17]
    out, state_out, weight_out, gain_out, hidden_out, split_out = refs[17:23]
    hv, hw, hr, tv, tw, tr, bias, rate, direct, pos, norm = held = refs[23:34]
    scratch, sems = refs[34:]
    copies = start_all(
        list(zip(sources, held))
        + [(gain, gain_out), (hidden, hidden_out), (state.at[0], state_out), (weight.at[0], weight_out)],
        sems,
    )
    for copy in copies[: len(held)]:
        copy.wait()
    layers, depth = hv.shape[:2]
    for layer in range(layers):
        taps = [ref[layer].astype(f32) for ref in (tv, tw, tr)]
        out[layer, 0:chunks] = pack(taps[0][depth : depth + 1])
        out[layer, chunks : 2 * chunks] = jnp.concatenate(
            [pack(taps[1][depth : depth + 1]), pack(taps[2][depth : depth + 1])], axis=0
        )
        out[layer, 2 * chunks : 3 * chunks] = interleave(
            scratch, column(direct[layer : layer + 1, :], heads)
        )
        out[layer, 3 * chunks : 4 * chunks] = pack(norm[layer : layer + 1, :])
        at = 4 * chunks
        out[layer, at : at + heads] = column(bias[layer : layer + 1, :], heads)
        at += heads
        out[layer, at : at + heads] = -jnp.exp(column(rate[layer : layer + 1, :], heads))
        at += heads
        for s in range(seqs):
            position = lengths_ref[s] - 1
            sums = []
            for ref, tap in zip((hv, hw, hr), taps):
                total = None
                for k in range(depth):
                    term = ref[layer, k].astype(f32)[s : s + 1] * tap[k : k + 1]
                    term = jnp.where(depth - position <= k, term, 0.0)
                    total = term if total is None else total + term
                sums.append(pack(total))
            out[layer, at : at + chunks] = sums[0]
            at += chunks
            out[layer, at : at + chunks] = jnp.concatenate(sums[1:], axis=0)
            at += chunks
            logs = pos[layer]
            here = jnp.sum(jnp.where(lane_iota(logs.shape) == position, logs, 0.0), axis=1, keepdims=True)
            out[layer, at : at + heads] = jnp.where(
                position > 0, jnp.broadcast_to(here, (heads, LANES)), -1e30
            )
            at += heads
    for copy in copies[len(held) : -1]:
        copy.wait()
    split_state(state_out, split_out)
    copies[-1].wait()


def two_terms(x):
    high = x.astype(bf16)
    return high, (x - high.astype(f32)).astype(bf16)


def split_state(held, out):
    seqs, heads, depth, _ = held.shape
    for s in range(seqs):
        for h in range(heads):
            high, rest = two_terms(held[s, h])
            at = (s * heads + h) * depth
            out[at : at + depth, 0:LANES] = high
            out[at : at + depth, LANES : 2 * LANES] = rest


def fetch_state_kernel(layer, *refs):
    state, weight, held, weight_out, split_out, sems = refs[1:]
    copies = start_all(halves(state.at[layer], held) + halves(weight.at[layer], weight_out), sems)
    copies[0].wait()
    copies[1].wait()
    split_state(held, split_out)
    copies[2].wait()
    copies[3].wait()


def fetch_kernel(plan, *refs):
    count = len(plan)
    sources, targets, sems = refs[1 : 1 + count], refs[1 + count : 1 + 2 * count], refs[-1]
    pairs = []
    for block, source, target in zip(plan, sources, targets):
        pairs += halves(source if block is None else source.at[block], target)
    for copy in start_all(pairs, sems):
        copy.wait()


def update_kernel(dims, layer, *refs):
    seqs, chunks, shared, heads, _, _ = dims
    lead_ref, acts, decays, held = refs[:4]
    out, made, sems = refs[-3:]
    per_group = heads // shared
    half = LANES // 2
    lead = lead_ref[...]
    count = lead.shape[0]
    high, rest = two_terms(lead)
    last = lead - high.astype(f32) - rest.astype(f32)
    terms = [high.astype(f32)] * 3 + [rest.astype(f32)] * 2 + [last]
    blank = jnp.zeros((LANES - 6 * count, LANES), f32)
    left = jnp.transpose(jnp.concatenate(terms + [blank], axis=0)).astype(bf16)
    at_row = lax.broadcasted_iota(jnp.int32, (count, LANES), 0)
    copies = []
    for s in range(seqs):
        for g in range(shared):
            write = acts[s, g : g + 1, :]
            high, rest = two_terms(write)
            last = write - high.astype(f32) - rest.astype(f32)
            high, rest = high.astype(f32), rest.astype(f32)
            right = []
            for i in range(per_group // 2):
                here = at_row == s * chunks + g * per_group // 2 + i
                terms = [jnp.where(here, jnp.broadcast_to(t, (count, LANES)), 0.0) for t in (high, rest, last)]
                order = [terms[0], terms[1], terms[2], terms[0], terms[1], terms[0], blank]
                right.append(jnp.concatenate(order, axis=0).astype(bf16))
            added = jnp.dot(left, jnp.concatenate(right, axis=1), preferred_element_type=f32)
            for i in range(per_group // 2):
                for j in range(2):
                    h = g * per_group + 2 * i + j
                    made[s, h] = (
                        decays[s, h : h + 1, :] * held[s, h]
                        + added[j * half : (j + 1) * half, i * LANES : (i + 1) * LANES]
                    )
            copy = pltpu.make_async_copy(
                made.at[s, pl.ds(g * per_group, per_group)],
                out.at[layer, s, pl.ds(g * per_group, per_group)],
                sems.at[s * shared + g],
            )
            copy.start()
            copies.append(copy)
    for copy in copies:
        copy.wait()


def silu(x):
    return x / (1.0 + jnp.exp(-x))


def mix_kernel(dims, layer, *refs):
    seqs, chunks, shared, heads, rows, fan = dims
    parts, table, split = refs[:fan], refs[fan], refs[fan + 1]
    gated_ref, rows_ref, lead_ref, acts, decays, pairs = refs[fan + 2 :]
    groups = shared
    per_group = heads // groups
    span = per_group // 2
    total = tree_sum([part[...] for part in parts])
    at_row = lax.broadcasted_iota(jnp.int32, (chunks, LANES), 0)
    for s in range(seqs):
        block = total[s * rows : (s + 1) * rows]
        at = 4 * chunks + 2 * heads + s * (2 * chunks + heads)
        last = block[2 * chunks + 2 * shared : 2 * chunks + 2 * shared + 1]
        scale = lax.rsqrt(last[:, LANES // 2 : LANES // 2 + 1] / D + epsilon)
        share_row = (block[2 * chunks : 2 * chunks + 2 * shared] * scale).astype(bf16).astype(f32)
        act = silu(
            share_row * table[layer, chunks : 2 * chunks]
            + table[layer, at + chunks : at + chunks + 2 * shared]
        )
        acts[s] = act
        sums = jnp.zeros((chunks, LANES), f32)
        write_rows, read_rows = [], []
        for g in range(groups):
            read = act[groups + g : groups + g + 1]
            here = (at_row >= g * span) & (at_row < (g + 1) * span)
            high, rest = two_terms(jnp.where(here, jnp.broadcast_to(read, (chunks, LANES)), 0.0))
            left = jnp.concatenate([high.astype(f32), rest.astype(f32)], axis=0).astype(bf16)
            size = span * LANES
            first = (s * groups + g) * size
            product = lax.dot_general(
                jnp.concatenate([left, left], axis=1),
                split[first : first + size, :],
                (((1,), (1,)), ((), ())),
                preferred_element_type=f32,
            )
            product = product[0:chunks] + product[chunks : 2 * chunks]
            for i in range(span):
                sums = jnp.where(at_row == g * span + i, product[:, i * LANES : (i + 1) * LANES], sums)
            write_rows += [act[g : g + 1]] * span
            read_rows += [read] * span
        overlap = jnp.sum(
            jnp.concatenate(write_rows, axis=0) * jnp.concatenate(read_rows, axis=0), axis=1, keepdims=True
        )
        gate = silu(block[0:chunks] * scale)
        value_row = (block[chunks : 2 * chunks] * scale).astype(bf16).astype(f32)
        rows_ref[s, 0:chunks] = value_row
        rows_ref[s, chunks : chunks + 2 * shared] = share_row
        value_act = silu(value_row * table[layer, 0:chunks] + table[layer, at : at + chunks])
        raw = column(last * scale, heads) + table[layer, 4 * chunks : 4 * chunks + heads]
        step = jnp.maximum(raw, 0.0) + jnp.log1p(jnp.exp(-jnp.abs(raw)))
        decay = jnp.exp(
            table[layer, 4 * chunks + heads : 4 * chunks + 2 * heads] * step
            + table[layer, at + 2 * chunks : at + 2 * chunks + heads]
        )
        decays[s] = decay
        lead = interleave(pairs.at[2 * s], step) * value_act
        lead_ref[s * chunks : (s + 1) * chunks, :] = lead
        readout = interleave(pairs.at[2 * s + 1], decay) * sums + lead * overlap
        mixed = (readout + table[layer, 2 * chunks : 3 * chunks] * value_act) * gate
        power = jnp.broadcast_to(jnp.sum(mixed * mixed, axis=1, keepdims=True), (chunks, LANES))
        other = jnp.where(
            lax.rem(at_row, 2) == 0, pltpu.roll(power, chunks - 1, 0), pltpu.roll(power, 1, 0)
        )
        mixed = mixed * lax.rsqrt((power + other) / (2 * LANES) + epsilon)
        gated_ref[s * chunks : (s + 1) * chunks, :] = (
            mixed * table[layer, 3 * chunks : 4 * chunks]
        ).astype(bf16)


def output_kernel(dims, *refs):
    seqs, chunks, _, _, _, fan = dims
    parts, weight = refs[:fan], refs[fan]
    out, scratch = refs[fan + 2 :]
    me = lax.axis_index("dp")
    block = seqs * chunks
    for mask in range(fan):
        start = pl.multiple_of(lax.bitwise_xor(me, jnp.int32(mask)) * block, block)
        scratch[pl.ds(start, block), :] = parts[mask][...].astype(f32)
    whole = jnp.concatenate(
        [scratch[pl.ds(c, fan * seqs, stride=chunks), :] for c in range(chunks)], axis=1
    ).astype(bf16)
    out[...] = jnp.dot(whole, weight[...], preferred_element_type=f32)


def close_kernel(x_ref, *refs):
    out = refs[-1]
    out[...] = (x_ref[...].astype(f32) + tree_sum([ref[...] for ref in refs[:-1]])).astype(bf16)


def buffer_kernel(dims, layers, *refs):
    seqs, chunks, shared, _, _, _ = dims
    new_rows = refs[1 : 1 + layers]
    past = refs[1 + layers : 4 + layers]
    outs = refs[4 + layers : 7 + layers]
    held = refs[7 + layers : 10 + layers]
    built = refs[10 + layers : 13 + layers]
    sems = refs[-1]
    for copy in start_all(list(zip(past, held)), sems):
        copy.wait()
    spans = ((0, chunks), (chunks, chunks + shared), (chunks + shared, chunks + 2 * shared))
    for old, new, (low, high) in zip(held, built, spans):
        depth = old.shape[1]
        for layer in range(layers):
            for k in range(depth - 1):
                new[layer, k] = old[layer, k + 1]
            new[layer, depth - 1] = jnp.concatenate(
                [unpack(new_rows[layer][s, low:high]) for s in range(seqs)], axis=0
            ).astype(bf16)
    for copy in start_all(list(zip(built, outs)), sems):
        copy.wait()


def full(memory=VMEM):
    return pl.BlockSpec(memory_space=memory)


HBM = pltpu.HBM


def place(arrays, memory):
    return [pltpu.with_memory_space_constraint(array, memory) for array in arrays]


def cost(flops, moved):
    return pl.CostEstimate(flops=flops, bytes_accessed=moved, transcendentals=0)


def direct(axis):
    size = lax.axis_size(axis)
    return size <= 8 and size & (size - 1) == 0


def swap(array, axis, mask):
    return lax.ppermute(array, axis, [(i, i ^ mask) for i in range(lax.axis_size(axis))])


def swaps(array, axis):
    return [array] + [swap(array, axis, mask) for mask in range(1, lax.axis_size(axis))]


def on_device_kernels(
    hidden,
    lengths,
    input_norm_gain,
    gate_matrix,
    input_matrix,
    write_matrix,
    read_matrix,
    step_matrix,
    step_size_bias,
    log_decay_rate,
    direct_path_gain,
    input_filter_taps,
    write_filter_taps,
    read_filter_taps,
    position_log_decay,
    grouped_norm_gain,
    output_matrix,
    recurrent_head_state,
    history_input_rows,
    history_write_rows,
    history_read_rows,
):
    layers, seqs, heads = recurrent_head_state.shape[:3]
    chunks = input_filter_taps.shape[2] // LANES
    shared = write_filter_taps.shape[2] // LANES
    rows = -(-(2 * chunks + 2 * shared + 1) // 8) * 8
    fan = lax.axis_size("dp")
    dims = (seqs, chunks, shared, heads, rows, fan)
    count = hidden.shape[0]
    weights = (
        gate_matrix,
        input_matrix,
        write_matrix,
        read_matrix,
        jnp.swapaxes(step_matrix, 1, 2),
    )
    past = [
        jnp.swapaxes(h, 1, 2) for h in (history_input_rows, history_write_rows, history_read_rows)
    ]
    state = recurrent_head_state
    params = pltpu.CompilerParams(vmem_limit_bytes=12 * 1024 * 1024)
    table_rows = 4 * chunks + 2 * heads + seqs * (2 * chunks + heads)
    message = pltpu.VMEM((seqs * rows, LANES), f32)
    pool = pltpu.VMEM((rows * count, LANES), f32)

    def fetch(after, blocks):
        sources = [array for array, _ in blocks]
        plan = [block for _, block in blocks]
        return pl.pallas_call(
            functools.partial(fetch_kernel, plan),
            out_shape=[
                pltpu.VMEM(a.shape if block is None else a.shape[1:], a.dtype) for a, block in blocks
            ],
            in_specs=[full()] + [full(HBM)] * len(blocks),
            out_specs=[full()] * len(blocks),
            scratch_shapes=[pltpu.SemaphoreType.DMA((2 * len(blocks),))],
            compiler_params=params,
            cost_estimate=cost(4_000_000, 1_000_000),
        )(*place([after], VMEM), *place(sources, HBM))

    def fetch_state(layer, after):
        return pl.pallas_call(
            functools.partial(fetch_state_kernel, layer),
            out_shape=[
                pltpu.VMEM(state.shape[1:], f32),
                pltpu.VMEM(output_matrix.shape[1:], bf16),
                pltpu.VMEM((seqs * heads * state.shape[3], 2 * LANES), bf16),
            ],
            in_specs=[full()] + [full(HBM)] * 2,
            out_specs=[full()] * 3,
            scratch_shapes=[pltpu.SemaphoreType.DMA((4,))],
            compiler_params=params,
            cost_estimate=cost(4_000_000, 1_000_000),
            name="fetch",
        )(*place([after], VMEM), *place([state, output_matrix], HBM))

    def mix(layer, parts, tables, split):
        return pl.pallas_call(
            functools.partial(mix_kernel, dims, layer),
            out_shape=[
                pltpu.VMEM((seqs * chunks, LANES), bf16),
                pltpu.VMEM((seqs, chunks + 2 * shared, LANES), f32),
                pltpu.VMEM((seqs * chunks, LANES), f32),
                pltpu.VMEM((seqs, 2 * shared, LANES), f32),
                pltpu.VMEM((seqs, heads, LANES), f32),
            ],
            in_specs=[full()] * (fan + 2),
            out_specs=[full()] * 5,
            scratch_shapes=[pltpu.VMEM((2 * seqs, heads, LANES), f32)],
            compiler_params=params,
            name="mix",
        )(*place(list(parts) + [tables, split], VMEM))

    def update(layer, factors, held, states):
        given = place([*factors, held], VMEM)
        if states is not None:
            given += place([states], HBM)
        return pl.pallas_call(
            functools.partial(update_kernel, dims, layer),
            out_shape=jax.ShapeDtypeStruct(state.shape, f32),
            in_specs=[full()] * 4 + [full(HBM)] * (len(given) - 4),
            out_specs=full(HBM),
            scratch_shapes=[
                pltpu.VMEM(state.shape[1:], f32),
                pltpu.SemaphoreType.DMA((seqs * shared,)),
            ],
            input_output_aliases={4: 0} if states is not None else {},
            compiler_params=params,
            cost_estimate=cost(4_000_000, 1_000_000),
            name="update",
        )(*given)

    def output(parts, weight, states):
        return pl.pallas_call(
            functools.partial(output_kernel, dims),
            out_shape=pltpu.VMEM((count, output_matrix.shape[2]), f32),
            in_specs=[full()] * (fan + 1) + [full(HBM)],
            out_specs=full(),
            scratch_shapes=[pltpu.VMEM((fan * seqs * chunks, LANES), f32)],
            compiler_params=params,
            name="output",
        )(*place(list(parts) + [weight], VMEM), *place([states], HBM))

    given = [hidden, input_norm_gain, *weights]
    made = pl.pallas_call(
        functools.partial(first_project_kernel, dims, 0),
        out_shape=[message] * fan,
        in_specs=[full(HBM) for _ in given],
        out_specs=[full()] * fan,
        scratch_shapes=[pltpu.VMEM(hidden.shape, bf16), pltpu.VMEM(input_norm_gain.shape, f32)]
        + [pltpu.VMEM(w.shape[1:], bf16) for w in weights]
        + [pool, pltpu.SemaphoreType.DMA((12,))],
        compiler_params=params,
        name="project",
    )(*place(given, HBM))
    small = past + [
        input_filter_taps,
        write_filter_taps,
        read_filter_taps,
        step_size_bias,
        log_decay_rate,
        direct_path_gain,
        jnp.swapaxes(position_log_decay, 1, 2),
        grouped_norm_gain,
    ]
    tables, held, weight, gain, stream, split = pl.pallas_call(
        functools.partial(table_kernel, dims),
        out_shape=[
            pltpu.VMEM((layers, table_rows, LANES), f32),
            pltpu.VMEM(state.shape[1:], f32),
            pltpu.VMEM(output_matrix.shape[1:], bf16),
            pltpu.VMEM(input_norm_gain.shape, f32),
            pltpu.VMEM(hidden.shape, bf16),
            pltpu.VMEM((seqs * heads * state.shape[3], 2 * LANES), bf16),
        ],
        in_specs=[full(pltpu.SMEM), full()] + [full(HBM)] * (len(small) + 4),
        out_specs=[full()] * 6,
        scratch_shapes=[pltpu.VMEM(a.shape, a.dtype) for a in small]
        + [pltpu.VMEM((heads, LANES), f32), pltpu.SemaphoreType.DMA((len(small) + 4,))],
        compiler_params=params,
        cost_estimate=cost(4_000_000, 1_000_000),
        name="tables",
    )(
        lengths,
        *place([made[0]], VMEM),
        *place(small + [state, output_matrix, input_norm_gain, hidden], HBM),
    )
    states = None
    new_rows = []
    for layer in range(layers):
        parts = [made[0]] + [swap(made[mask], "dp", mask) for mask in range(1, fan)]
        if layer > 0:
            held, weight, split = fetch_state(layer, made[0])
        gated, row_values, *factors = mix(layer, parts, tables, split)
        new_rows.append(row_values)
        parts = swaps(gated, "dp")
        states = update(layer, factors, held, states)
        own = output(parts, weight, states)
        partial = swaps(own, "tp")
        if layer + 1 < layers:
            ahead = fetch(own, [(w, layer + 1) for w in weights])
            stream, *made = pl.pallas_call(
                functools.partial(next_project_kernel, dims, layer + 1),
                out_shape=[pltpu.VMEM(hidden.shape, bf16)] + [message] * fan,
                in_specs=[full()] * (2 + len(partial) + len(weights)),
                out_specs=[full()] * (1 + fan),
                scratch_shapes=[pool],
                compiler_params=params,
                name="project",
            )(*place([stream, *partial, gain, *ahead], VMEM))
    buffers = pl.pallas_call(
        functools.partial(buffer_kernel, dims, layers),
        out_shape=[jax.ShapeDtypeStruct(h.shape, bf16) for h in past],
        in_specs=[full()] * (1 + layers) + [full(HBM)] * 3,
        out_specs=[full(HBM)] * 3,
        scratch_shapes=[pltpu.VMEM(h.shape, bf16) for h in past] * 2 + [pltpu.SemaphoreType.DMA((3,))],
        compiler_params=params,
        cost_estimate=cost(4_000_000, 1_000_000),
        name="buffers",
    )(*place([own] + new_rows, VMEM), *place(past, HBM))
    buffers = [jnp.swapaxes(b, 1, 2) for b in buffers]
    stream = pl.pallas_call(
        close_kernel,
        out_shape=jax.ShapeDtypeStruct(hidden.shape, bf16),
        in_specs=[full()] * (1 + len(partial)),
        out_specs=full(),
        compiler_params=params,
        name="close",
    )(*place([stream, *partial], VMEM))
    return (stream, states, *buffers)


def kernels_fit(state, taps, write_taps, hidden, output_matrix, step_matrix):
    _, seqs, heads, head_dim, state_dim = state.shape
    shared = write_taps.shape[2] // LANES
    chunks = taps.shape[2] // LANES
    return (
        direct("dp")
        and direct("tp")
        and state_dim == LANES
        and head_dim * 2 == LANES
        and shared > 0
        and heads == 4 * shared
        and chunks == 2 * shared
        and chunks % 8 == 0
        and heads % 16 == 0
        and seqs * chunks <= LANES
        and seqs * chunks % 16 == 0
        and hidden.shape[0] == seqs * lax.axis_size("dp")
        and hidden.shape[0] % 8 == 0
        and hidden.shape[1] % LANES == 0
        and output_matrix.shape[2] % LANES == 0
        and step_matrix.shape[2] <= LANES
        and heads <= LANES // 2
    )


def convolve(buffer, new_row, weights, tap_valid):
    tap_rows = weights.astype(jnp.float32)
    depth = weights.shape[0] - 1
    summed = new_row.astype(jnp.float32) * tap_rows[depth]
    for k in range(depth):
        summed = summed + buffer[:, k].astype(jnp.float32) * tap_rows[k] * tap_valid[:, k : k + 1]
    shifted = jnp.concatenate([buffer[:, 1:], new_row[:, None]], axis=1)
    return (jax.nn.silu(summed), shifted)


def spread_groups(rows, seq_local, groups_local, per_group, state_dim):
    grouped = rows.reshape(seq_local, groups_local, 1, state_dim)
    return jnp.broadcast_to(grouped, (seq_local, groups_local, per_group, state_dim)).reshape(
        seq_local, groups_local * per_group, state_dim
    )


def exchange_rows(rows, axis, count):
    if not direct(axis):
        return lax.psum_scatter(rows, axis, scatter_dimension=0, tiled=True)
    me = lax.axis_index(axis)
    parts = [
        lax.dynamic_slice_in_dim(rows, (me ^ mask) * count, count, 0)
        for mask in range(lax.axis_size(axis))
    ]
    return tree_sum([parts[0]] + [swap(parts[mask], axis, mask) for mask in range(1, len(parts))])


def gather_rows(rows, axis):
    if not direct(axis):
        return lax.all_gather(rows, axis, axis=0, tiled=True)
    me, size = lax.axis_index(axis), lax.axis_size(axis)
    parts = [rows] + [swap(rows, axis, mask) for mask in range(1, size)]
    whole = jnp.zeros((size,) + rows.shape, rows.dtype)
    for mask in range(size):
        whole = lax.dynamic_update_index_in_dim(whole, parts[mask], me ^ mask, 0)
    return whole.reshape((size * rows.shape[0],) + rows.shape[1:])


def sum_copies(rows, axis):
    if not direct(axis):
        return lax.psum(rows, axis)
    return tree_sum([rows] + [swap(rows, axis, mask) for mask in range(1, lax.axis_size(axis))])


def on_device_plain(
    hidden,
    lengths,
    input_norm_gain,
    gate_matrix,
    input_matrix,
    write_matrix,
    read_matrix,
    step_matrix,
    step_size_bias,
    log_decay_rate,
    direct_path_gain,
    input_filter_taps,
    write_filter_taps,
    read_filter_taps,
    position_log_decay,
    grouped_norm_gain,
    output_matrix,
    recurrent_head_state,
    history_input_rows,
    history_write_rows,
    history_read_rows,
):
    seq_local = lengths.shape[0]
    heads_local = step_size_bias.shape[1]
    head_dim = recurrent_head_state.shape[3]
    state_dim = recurrent_head_state.shape[4]
    groups_local = write_filter_taps.shape[2] // state_dim
    per_group = heads_local // groups_local
    inner_local = heads_local * head_dim
    shared_local = groups_local * state_dim
    depth = input_filter_taps.shape[1] - 1
    token_position = lengths - 1
    tap_valid = (jnp.arange(depth)[None, :] >= depth - token_position[:, None]).astype(jnp.float32)
    state_is_valid = (token_position > 0).astype(jnp.float32)[:, None]
    position_indicator = (
        token_position[:, None] == jnp.arange(position_log_decay.shape[1])[None, :]
    ).astype(jnp.float32)
    head_first = lax.axis_index("tp") * heads_local
    stream = hidden
    states, values, writes, reads = ([], [], [], [])
    for layer_index in range(input_norm_gain.shape[0]):
        stream_float = stream.astype(jnp.float32)
        squares = jnp.sum(stream_float * stream_float, axis=1)
        normed = (stream_float * input_norm_gain[layer_index]).astype(jnp.bfloat16)
        pieces = [
            jnp.dot(normed, weight[layer_index], preferred_element_type=jnp.float32)
            for weight in (gate_matrix, input_matrix, write_matrix, read_matrix)
        ]
        step_term = jnp.dot(normed, step_matrix[layer_index], preferred_element_type=jnp.float32)
        heads_all = step_term.shape[1]
        width = sum(piece.shape[1] for piece in pieces)
        joined = jnp.concatenate(pieces + [step_term, squares[:, None]], axis=1)
        joined_mine = exchange_rows(joined, "dp", seq_local)
        mean_square = joined_mine[:, width + heads_all :] / D
        row_scale = lax.rsqrt(mean_square + epsilon)
        step_mine = joined_mine[:, width : width + heads_all]
        step_raw = lax.dynamic_slice_in_dim(step_mine, head_first, heads_local, 1) * row_scale
        scaled = joined_mine[:, :width] * row_scale
        proj_gate = scaled[:, :inner_local]
        value_row = scaled[:, inner_local : 2 * inner_local].astype(jnp.bfloat16)
        write_row = scaled[:, 2 * inner_local : 2 * inner_local + shared_local].astype(jnp.bfloat16)
        read_row = scaled[:, 2 * inner_local + shared_local :].astype(jnp.bfloat16)
        value_act, value_buf = convolve(
            history_input_rows[layer_index], value_row, input_filter_taps[layer_index], tap_valid
        )
        write_act, write_buf = convolve(
            history_write_rows[layer_index], write_row, write_filter_taps[layer_index], tap_valid
        )
        read_act, read_buf = convolve(
            history_read_rows[layer_index], read_row, read_filter_taps[layer_index], tap_valid
        )
        head_step_size = jax.nn.softplus(step_raw + step_size_bias[layer_index])
        current_log_decay = jnp.dot(
            position_indicator, position_log_decay[layer_index], precision=lax.Precision.HIGHEST
        )
        current_decay = (
            jnp.exp(-jnp.exp(log_decay_rate[layer_index]) * head_step_size + current_log_decay)
            * state_is_valid
        )
        value_heads = value_act.reshape(seq_local, heads_local, head_dim)
        write_heads = spread_groups(write_act, seq_local, groups_local, per_group, state_dim)
        read_heads = spread_groups(read_act, seq_local, groups_local, per_group, state_dim)
        updated = (
            current_decay[:, :, None, None] * recurrent_head_state[layer_index]
            + (head_step_size[:, :, None] * value_heads)[:, :, :, None] * write_heads[:, :, None, :]
        )
        readout = jnp.einsum("shpn,shn->shp", updated, read_heads, precision=lax.Precision.HIGHEST)
        mixed_heads = (
            readout + direct_path_gain[layer_index][None, :, None] * value_heads
        ) * jax.nn.silu(proj_gate.reshape(seq_local, heads_local, head_dim))
        grouped = mixed_heads.reshape(seq_local, groups_local, per_group * head_dim)
        grouped = grouped * lax.rsqrt(jnp.mean(grouped * grouped, axis=2, keepdims=True) + epsilon)
        gated_rows = (
            grouped.reshape(seq_local, inner_local) * grouped_norm_gain[layer_index]
        ).astype(jnp.bfloat16)
        out_weight = output_matrix[layer_index]

        gathered = gather_rows(gated_rows, "dp")
        partial_out = jnp.dot(gathered, out_weight, preferred_element_type=jnp.float32)
        branch = sum_copies(partial_out, "tp")
        stream = (stream_float + branch).astype(jnp.bfloat16)
        states.append(updated)
        values.append(value_buf)
        writes.append(write_buf)
        reads.append(read_buf)
    return (stream, jnp.stack(states), jnp.stack(values), jnp.stack(writes), jnp.stack(reads))


def on_device(*args):
    hidden, taps, write_taps = args[0], args[11], args[12]
    if kernels_fit(args[17], taps, write_taps, hidden, args[16], args[7]):
        return on_device_kernels(*args)
    return on_device_plain(*args)


def solution(mesh):
    placed = (
        P("grp", "dp"),
        P(("grp", "dp")),
        P(None, "dp"),
        P(None, "dp", "tp"),
        P(None, "dp", "tp"),
        P(None, "dp", "tp"),
        P(None, "dp", "tp"),
        P(None, "dp", None),
        P(None, "tp"),
        P(None, "tp"),
        P(None, "tp"),
        P(None, None, "tp"),
        P(None, None, "tp"),
        P(None, None, "tp"),
        P(None, None, "tp"),
        P(None, "tp"),
        P(None, "tp", "dp"),
        P(None, ("grp", "dp"), "tp", None, None),
        P(None, ("grp", "dp"), None, "tp"),
        P(None, ("grp", "dp"), None, "tp"),
        P(None, ("grp", "dp"), None, "tp"),
    )
    return jax.shard_map(
        on_device,
        mesh=mesh,
        in_specs=placed,
        out_specs=(
            P("grp", "dp"),
            P(None, ("grp", "dp"), "tp", None, None),
            P(None, ("grp", "dp"), None, "tp"),
            P(None, ("grp", "dp"), None, "tp"),
            P(None, ("grp", "dp"), None, "tp"),
        ),
        check_vma=False,
    )
```

```python
import functools

import jax
import jax.numpy as jnp
from jax import lax
from jax.experimental import pallas as pl
from jax.experimental.pallas import tpu as pltpu
from jax.sharding import PartitionSpec as P


D = 2048


epsilon = 1e-06
LANES = 128
LINE = ((1, 3, 0, 2), (3, 2, 1, 0), (2, 0, 3, 1))
LINE_LAST = ((3, 2, 1, 0), (2, 3, 0, 1), (1, 0, 3, 2))
f32 = jnp.float32
bf16 = jnp.bfloat16
VMEM = pltpu.VMEM


def lane_iota(shape):
    return lax.broadcasted_iota(jnp.int32, shape, 1)


def pack(row):
    return jnp.concatenate(
        [row[:, i : i + LANES] for i in range(0, row.shape[1], LANES)], axis=0
    )


def unpack(rows):
    return jnp.concatenate([rows[i : i + 1] for i in range(rows.shape[0])], axis=1)


def column(row, count):
    wide = jnp.broadcast_to(row[:, :count], (count, count))
    eye = lane_iota((count, count)) == lax.broadcasted_iota(jnp.int32, (count, count), 0)
    return jnp.broadcast_to(
        jnp.sum(jnp.where(eye, wide, 0.0), axis=1, keepdims=True), (count, LANES)
    )


def interleave(scratch, rows):
    half = rows.shape[0] // 2
    scratch[...] = rows
    even = scratch[pl.ds(0, half, stride=2), :]
    odd = scratch[pl.ds(1, half, stride=2), :]
    return jnp.where(lane_iota((half, LANES)) < LANES // 2, even, odd)


def tree_sum(parts):
    while len(parts) > 1:
        parts = [parts[i] + parts[i + 1] for i in range(0, len(parts), 2)]
    return parts[0]


def start_all(pairs, sems):
    copies = [pltpu.make_async_copy(source, target, sems.at[i]) for i, (source, target) in enumerate(pairs)]
    for copy in copies:
        copy.start()
    return copies


def halves(source, target, count=2):
    size = target.shape[0] // count
    return [
        (source.at[pl.ds(i * size, size)], target.at[pl.ds(i * size, size)]) for i in range(count)
    ]


def project_rows(dims, x, gain, held, waits, outs, scratch):
    seqs, _, _, heads, rows, fan = dims
    squares = jnp.sum(x * x, axis=1, keepdims=True)
    normed = (x * gain).astype(bf16)
    count = x.shape[0]
    base = 0
    for i in range(4):
        for copy in waits[i]:
            copy.wait()
        piece = jnp.dot(normed, held[i][...], preferred_element_type=f32)
        for c in range(piece.shape[1] // LANES):
            scratch[pl.ds((base + c) * count, count), :] = piece[:, c * LANES : (c + 1) * LANES]
        base += piece.shape[1] // LANES
    for copy in waits[4]:
        copy.wait()
    step = lax.dot_general(
        normed, held[4][...], (((1,), (1,)), ((), ())), preferred_element_type=f32
    )
    width = step.shape[1]
    if width < LANES:
        step = jnp.concatenate([step, jnp.zeros((count, LANES - width), f32)], axis=1)
    shift = lax.rem(LANES - lax.axis_index("tp") * heads, LANES)
    step = pltpu.roll(step, shift, 1)
    last = jnp.where(lane_iota((count, LANES)) < heads, step, jnp.broadcast_to(squares, (count, LANES)))
    scratch[pl.ds(base * count, count), :] = last
    for i in range(base + 1, rows):
        scratch[pl.ds(i * count, count), :] = jnp.zeros((count, LANES), f32)
    me = lax.axis_index("dp")
    for mask in range(fan):
        first = lax.bitwise_xor(me, jnp.int32(mask)) * seqs
        for s in range(seqs):
            outs[mask][pl.ds(s * rows, rows), :] = scratch[pl.ds(first + s, rows, stride=count), :]


def first_project_kernel(dims, layer, *refs):
    fan = dims[5]
    refs = list(refs)
    x_hbm, gain_hbm = refs[:2]
    weights = refs[2:7]
    outs = refs[7 : 7 + fan]
    x_ref, gain_ref = refs[7 + fan : 9 + fan]
    held = refs[9 + fan : 14 + fan]
    scratch, sems = refs[14 + fan :]
    pairs = [(x_hbm, x_ref), (gain_hbm, gain_ref)]
    spans = []
    for source, target in zip(weights, held):
        more = halves(source.at[layer], target)
        spans.append((len(pairs), len(pairs) + len(more)))
        pairs += more
    copies = start_all(pairs, sems)
    copies[0].wait()
    copies[1].wait()
    waits = [copies[low:high] for low, high in spans]
    project_rows(
        dims, x_ref[...].astype(f32), gain_ref[layer : layer + 1, :], held, waits, outs, scratch
    )


def next_project_kernel(dims, layer, *refs):
    fan, tp = dims[5], lax.axis_size("tp")
    refs = list(refs)
    x_ref, parts, gain_ref = refs[0], refs[1 : 1 + tp], refs[1 + tp]
    held = refs[2 + tp : 7 + tp]
    new_ref = refs[7 + tp]
    outs = refs[8 + tp : 8 + tp + fan]
    scratch = refs[-1]
    new = (x_ref[...].astype(f32) + tree_sum([part[...] for part in parts])).astype(bf16)
    new_ref[...] = new
    project_rows(
        dims, new.astype(f32), gain_ref[layer : layer + 1, :], held, [[]] * 5, outs, scratch
    )


def table_kernel(dims, *refs):
    seqs, chunks, _, heads, _, _ = dims
    lengths_ref = refs[0]
    sources = refs[2:13]
    state, weight, gain, hidden = refs[13:17]
    out, state_out, weight_out, gain_out, hidden_out, split_out = refs[17:23]
    hv, hw, hr, tv, tw, tr, bias, rate, direct, pos, norm = held = refs[23:34]
    scratch, sems = refs[34:]
    copies = start_all(
        list(zip(sources, held))
        + [(gain, gain_out), (hidden, hidden_out), (state.at[0], state_out), (weight.at[0], weight_out)],
        sems,
    )
    for copy in copies[: len(held)]:
        copy.wait()
    layers, depth = hv.shape[:2]
    for layer in range(layers):
        taps = [ref[layer].astype(f32) for ref in (tv, tw, tr)]
        out[layer, 0:chunks] = pack(taps[0][depth : depth + 1])
        out[layer, chunks : 2 * chunks] = jnp.concatenate(
            [pack(taps[1][depth : depth + 1]), pack(taps[2][depth : depth + 1])], axis=0
        )
        out[layer, 2 * chunks : 3 * chunks] = interleave(
            scratch, column(direct[layer : layer + 1, :], heads)
        )
        out[layer, 3 * chunks : 4 * chunks] = pack(norm[layer : layer + 1, :])
        at = 4 * chunks
        out[layer, at : at + heads] = column(bias[layer : layer + 1, :], heads)
        at += heads
        out[layer, at : at + heads] = -jnp.exp(column(rate[layer : layer + 1, :], heads))
        at += heads
        for s in range(seqs):
            position = lengths_ref[s] - 1
            sums = []
            for ref, tap in zip((hv, hw, hr), taps):
                total = None
                for k in range(depth):
                    term = ref[layer, k].astype(f32)[s : s + 1] * tap[k : k + 1]
                    term = jnp.where(depth - position <= k, term, 0.0)
                    total = term if total is None else total + term
                sums.append(pack(total))
            out[layer, at : at + chunks] = sums[0]
            at += chunks
            out[layer, at : at + chunks] = jnp.concatenate(sums[1:], axis=0)
            at += chunks
            logs = pos[layer]
            here = jnp.sum(jnp.where(lane_iota(logs.shape) == position, logs, 0.0), axis=1, keepdims=True)
            out[layer, at : at + heads] = jnp.where(
                position > 0, jnp.broadcast_to(here, (heads, LANES)), -1e30
            )
            at += heads
    for copy in copies[len(held) : -1]:
        copy.wait()
    split_state(state_out, split_out)
    copies[-1].wait()


def two_terms(x):
    high = x.astype(bf16)
    return high, (x - high.astype(f32)).astype(bf16)


def split_state(held, out):
    seqs, heads, depth, _ = held.shape
    for s in range(seqs):
        for h in range(heads):
            high, rest = two_terms(held[s, h])
            at = (s * heads + h) * depth
            out[at : at + depth, 0:LANES] = high
            out[at : at + depth, LANES : 2 * LANES] = rest


def fetch_state_kernel(layer, *refs):
    state, weight, held, weight_out, split_out, sems = refs[1:]
    copies = start_all(halves(state.at[layer], held) + halves(weight.at[layer], weight_out), sems)
    copies[0].wait()
    copies[1].wait()
    split_state(held, split_out)
    copies[2].wait()
    copies[3].wait()


def fetch_kernel(plan, *refs):
    count = len(plan)
    sources, targets, sems = refs[1 : 1 + count], refs[1 + count : 1 + 2 * count], refs[-1]
    pairs = []
    for block, source, target in zip(plan, sources, targets):
        pairs += halves(source if block is None else source.at[block], target)
    for copy in start_all(pairs, sems):
        copy.wait()


def update_kernel(dims, layer, *refs):
    seqs, chunks, shared, heads, _, _ = dims
    lead_ref, acts, decays, held = refs[:4]
    out, made, sems = refs[-3:]
    per_group = heads // shared
    half = LANES // 2
    lead = lead_ref[...]
    count = lead.shape[0]
    high, rest = two_terms(lead)
    last = lead - high.astype(f32) - rest.astype(f32)
    terms = [high.astype(f32)] * 3 + [rest.astype(f32)] * 2 + [last]
    blank = jnp.zeros((LANES - 6 * count, LANES), f32)
    left = jnp.transpose(jnp.concatenate(terms + [blank], axis=0)).astype(bf16)
    at_row = lax.broadcasted_iota(jnp.int32, (count, LANES), 0)
    copies = []
    for s in range(seqs):
        for g in range(shared):
            write = acts[s, g : g + 1, :]
            high, rest = two_terms(write)
            last = write - high.astype(f32) - rest.astype(f32)
            high, rest = high.astype(f32), rest.astype(f32)
            right = []
            for i in range(per_group // 2):
                here = at_row == s * chunks + g * per_group // 2 + i
                terms = [jnp.where(here, jnp.broadcast_to(t, (count, LANES)), 0.0) for t in (high, rest, last)]
                order = [terms[0], terms[1], terms[2], terms[0], terms[1], terms[0], blank]
                right.append(jnp.concatenate(order, axis=0).astype(bf16))
            added = jnp.dot(left, jnp.concatenate(right, axis=1), preferred_element_type=f32)
            for i in range(per_group // 2):
                for j in range(2):
                    h = g * per_group + 2 * i + j
                    made[s, h] = (
                        decays[s, h : h + 1, :] * held[s, h]
                        + added[j * half : (j + 1) * half, i * LANES : (i + 1) * LANES]
                    )
            copy = pltpu.make_async_copy(
                made.at[s, pl.ds(g * per_group, per_group)],
                out.at[layer, s, pl.ds(g * per_group, per_group)],
                sems.at[s * shared + g],
            )
            copy.start()
            copies.append(copy)
    for copy in copies:
        copy.wait()


def silu(x):
    return x / (1.0 + jnp.exp(-x))


def mix_kernel(dims, layer, *refs):
    seqs, chunks, shared, heads, rows, fan = dims
    parts, table, split = refs[:fan], refs[fan], refs[fan + 1]
    gated_ref, rows_ref, lead_ref, acts, decays, pairs = refs[fan + 2 :]
    groups = shared
    per_group = heads // groups
    span = per_group // 2
    total = tree_sum([part[...] for part in parts])
    at_row = lax.broadcasted_iota(jnp.int32, (chunks, LANES), 0)
    for s in range(seqs):
        block = total[s * rows : (s + 1) * rows]
        at = 4 * chunks + 2 * heads + s * (2 * chunks + heads)
        last = block[2 * chunks + 2 * shared : 2 * chunks + 2 * shared + 1]
        scale = lax.rsqrt(last[:, LANES // 2 : LANES // 2 + 1] / D + epsilon)
        share_row = (block[2 * chunks : 2 * chunks + 2 * shared] * scale).astype(bf16).astype(f32)
        act = silu(
            share_row * table[layer, chunks : 2 * chunks]
            + table[layer, at + chunks : at + chunks + 2 * shared]
        )
        acts[s] = act
        sums = jnp.zeros((chunks, LANES), f32)
        write_rows, read_rows = [], []
        for g in range(groups):
            read = act[groups + g : groups + g + 1]
            here = (at_row >= g * span) & (at_row < (g + 1) * span)
            high, rest = two_terms(jnp.where(here, jnp.broadcast_to(read, (chunks, LANES)), 0.0))
            left = jnp.concatenate([high.astype(f32), rest.astype(f32)], axis=0).astype(bf16)
            size = span * LANES
            first = (s * groups + g) * size
            product = lax.dot_general(
                jnp.concatenate([left, left], axis=1),
                split[first : first + size, :],
                (((1,), (1,)), ((), ())),
                preferred_element_type=f32,
            )
            product = product[0:chunks] + product[chunks : 2 * chunks]
            for i in range(span):
                sums = jnp.where(at_row == g * span + i, product[:, i * LANES : (i + 1) * LANES], sums)
            write_rows += [act[g : g + 1]] * span
            read_rows += [read] * span
        overlap = jnp.sum(
            jnp.concatenate(write_rows, axis=0) * jnp.concatenate(read_rows, axis=0), axis=1, keepdims=True
        )
        gate = silu(block[0:chunks] * scale)
        value_row = (block[chunks : 2 * chunks] * scale).astype(bf16).astype(f32)
        rows_ref[s, 0:chunks] = value_row
        rows_ref[s, chunks : chunks + 2 * shared] = share_row
        value_act = silu(value_row * table[layer, 0:chunks] + table[layer, at : at + chunks])
        raw = column(last * scale, heads) + table[layer, 4 * chunks : 4 * chunks + heads]
        step = jnp.maximum(raw, 0.0) + jnp.log1p(jnp.exp(-jnp.abs(raw)))
        decay = jnp.exp(
            table[layer, 4 * chunks + heads : 4 * chunks + 2 * heads] * step
            + table[layer, at + 2 * chunks : at + 2 * chunks + heads]
        )
        decays[s] = decay
        lead = interleave(pairs.at[2 * s], step) * value_act
        lead_ref[s * chunks : (s + 1) * chunks, :] = lead
        readout = interleave(pairs.at[2 * s + 1], decay) * sums + lead * overlap
        mixed = (readout + table[layer, 2 * chunks : 3 * chunks] * value_act) * gate
        power = jnp.broadcast_to(jnp.sum(mixed * mixed, axis=1, keepdims=True), (chunks, LANES))
        other = jnp.where(
            lax.rem(at_row, 2) == 0, pltpu.roll(power, chunks - 1, 0), pltpu.roll(power, 1, 0)
        )
        mixed = mixed * lax.rsqrt((power + other) / (2 * LANES) + epsilon)
        gated_ref[s * chunks : (s + 1) * chunks, :] = (
            mixed * table[layer, 3 * chunks : 4 * chunks]
        ).astype(bf16)


def output_kernel(dims, *refs):
    seqs, chunks, _, _, _, fan = dims
    parts, weight = refs[:fan], refs[fan]
    out, scratch = refs[fan + 2 :]
    me = lax.axis_index("dp")
    block = seqs * chunks
    for mask in range(fan):
        start = pl.multiple_of(lax.bitwise_xor(me, jnp.int32(mask)) * block, block)
        scratch[pl.ds(start, block), :] = parts[mask][...].astype(f32)
    whole = jnp.concatenate(
        [scratch[pl.ds(c, fan * seqs, stride=chunks), :] for c in range(chunks)], axis=1
    ).astype(bf16)
    out[...] = jnp.dot(whole, weight[...], preferred_element_type=f32)


def close_kernel(x_ref, *refs):
    out = refs[-1]
    out[...] = (x_ref[...].astype(f32) + tree_sum([ref[...] for ref in refs[:-1]])).astype(bf16)


def buffer_kernel(dims, layers, *refs):
    seqs, chunks, shared, _, _, _ = dims
    new_rows = refs[1 : 1 + layers]
    past = refs[1 + layers : 4 + layers]
    outs = refs[4 + layers : 7 + layers]
    held = refs[7 + layers : 10 + layers]
    built = refs[10 + layers : 13 + layers]
    sems = refs[-1]
    for copy in start_all(list(zip(past, held)), sems):
        copy.wait()
    spans = ((0, chunks), (chunks, chunks + shared), (chunks + shared, chunks + 2 * shared))
    for old, new, (low, high) in zip(held, built, spans):
        depth = old.shape[1]
        for layer in range(layers):
            for k in range(depth - 1):
                new[layer, k] = old[layer, k + 1]
            new[layer, depth - 1] = jnp.concatenate(
                [unpack(new_rows[layer][s, low:high]) for s in range(seqs)], axis=0
            ).astype(bf16)
    for copy in start_all(list(zip(built, outs)), sems):
        copy.wait()


def full(memory=VMEM):
    return pl.BlockSpec(memory_space=memory)


HBM = pltpu.HBM


def place(arrays, memory):
    return [pltpu.with_memory_space_constraint(array, memory) for array in arrays]


def cost(flops, moved):
    return pl.CostEstimate(flops=flops, bytes_accessed=moved, transcendentals=0)


def direct(axis):
    size = lax.axis_size(axis)
    return size <= 8 and size & (size - 1) == 0


def swap(array, axis, mask):
    return lax.ppermute(array, axis, [(i, i ^ mask) for i in range(lax.axis_size(axis))])


def line_swaps(array, axis, rounds):
    got = []
    for targets in rounds:
        got.append(lax.ppermute(array, axis, list(enumerate(targets))))
    paired = [all(t[t[i]] == i for i in range(len(t))) for t in rounds].index(True)
    return [array, got[paired]] + got[:paired] + got[paired + 1 :]


def swaps(array, axis):
    return [array] + [swap(array, axis, mask) for mask in range(1, lax.axis_size(axis))]


def on_device_kernels(
    hidden,
    lengths,
    input_norm_gain,
    gate_matrix,
    input_matrix,
    write_matrix,
    read_matrix,
    step_matrix,
    step_size_bias,
    log_decay_rate,
    direct_path_gain,
    input_filter_taps,
    write_filter_taps,
    read_filter_taps,
    position_log_decay,
    grouped_norm_gain,
    output_matrix,
    recurrent_head_state,
    history_input_rows,
    history_write_rows,
    history_read_rows,
):
    layers, seqs, heads = recurrent_head_state.shape[:3]
    chunks = input_filter_taps.shape[2] // LANES
    shared = write_filter_taps.shape[2] // LANES
    rows = -(-(2 * chunks + 2 * shared + 1) // 4) * 4
    fan = lax.axis_size("dp")
    dims = (seqs, chunks, shared, heads, rows, fan)
    count = hidden.shape[0]
    weights = (
        gate_matrix,
        input_matrix,
        write_matrix,
        read_matrix,
        jnp.swapaxes(step_matrix, 1, 2),
    )
    past = [
        jnp.swapaxes(h, 1, 2) for h in (history_input_rows, history_write_rows, history_read_rows)
    ]
    state = recurrent_head_state
    params = pltpu.CompilerParams(vmem_limit_bytes=12 * 1024 * 1024)
    table_rows = 4 * chunks + 2 * heads + seqs * (2 * chunks + heads)
    message = pltpu.VMEM((seqs * rows, LANES), f32)
    pool = pltpu.VMEM((rows * count, LANES), f32)

    def fetch(after, blocks):
        sources = [array for array, _ in blocks]
        plan = [block for _, block in blocks]
        return pl.pallas_call(
            functools.partial(fetch_kernel, plan),
            out_shape=[
                pltpu.VMEM(a.shape if block is None else a.shape[1:], a.dtype) for a, block in blocks
            ],
            in_specs=[full()] + [full(HBM)] * len(blocks),
            out_specs=[full()] * len(blocks),
            scratch_shapes=[pltpu.SemaphoreType.DMA((2 * len(blocks),))],
            compiler_params=params,
            cost_estimate=cost(4_000_000, 1_000_000),
        )(*place([after], VMEM), *place(sources, HBM))

    def fetch_state(layer, after):
        return pl.pallas_call(
            functools.partial(fetch_state_kernel, layer),
            out_shape=[
                pltpu.VMEM(state.shape[1:], f32),
                pltpu.VMEM(output_matrix.shape[1:], bf16),
                pltpu.VMEM((seqs * heads * state.shape[3], 2 * LANES), bf16),
            ],
            in_specs=[full()] + [full(HBM)] * 2,
            out_specs=[full()] * 3,
            scratch_shapes=[pltpu.SemaphoreType.DMA((4,))],
            compiler_params=params,
            cost_estimate=cost(4_000_000, 1_000_000),
            name="fetch",
        )(*place([after], VMEM), *place([state, output_matrix], HBM))

    def mix(layer, parts, tables, split):
        return pl.pallas_call(
            functools.partial(mix_kernel, dims, layer),
            out_shape=[
                pltpu.VMEM((seqs * chunks, LANES), bf16),
                pltpu.VMEM((seqs, chunks + 2 * shared, LANES), f32),
                pltpu.VMEM((seqs * chunks, LANES), f32),
                pltpu.VMEM((seqs, 2 * shared, LANES), f32),
                pltpu.VMEM((seqs, heads, LANES), f32),
            ],
            in_specs=[full()] * (fan + 2),
            out_specs=[full()] * 5,
            scratch_shapes=[pltpu.VMEM((2 * seqs, heads, LANES), f32)],
            compiler_params=params,
            name="mix",
        )(*place(list(parts) + [tables, split], VMEM))

    def update(layer, factors, held, states):
        given = place([*factors, held], VMEM)
        if states is not None:
            given += place([states], HBM)
        return pl.pallas_call(
            functools.partial(update_kernel, dims, layer),
            out_shape=jax.ShapeDtypeStruct(state.shape, f32),
            in_specs=[full()] * 4 + [full(HBM)] * (len(given) - 4),
            out_specs=full(HBM),
            scratch_shapes=[
                pltpu.VMEM(state.shape[1:], f32),
                pltpu.SemaphoreType.DMA((seqs * shared,)),
            ],
            input_output_aliases={4: 0} if states is not None else {},
            compiler_params=params,
            cost_estimate=cost(4_000_000, 1_000_000),
            name="update",
        )(*given)

    def output(parts, weight, states):
        return pl.pallas_call(
            functools.partial(output_kernel, dims),
            out_shape=pltpu.VMEM((count, output_matrix.shape[2]), f32),
            in_specs=[full()] * (fan + 1) + [full(HBM)],
            out_specs=full(),
            scratch_shapes=[pltpu.VMEM((fan * seqs * chunks, LANES), f32)],
            compiler_params=params,
            name="output",
        )(*place(list(parts) + [weight], VMEM), *place([states], HBM))

    given = [hidden, input_norm_gain, *weights]
    made = pl.pallas_call(
        functools.partial(first_project_kernel, dims, 0),
        out_shape=[message] * fan,
        in_specs=[full(HBM) for _ in given],
        out_specs=[full()] * fan,
        scratch_shapes=[pltpu.VMEM(hidden.shape, bf16), pltpu.VMEM(input_norm_gain.shape, f32)]
        + [pltpu.VMEM(w.shape[1:], bf16) for w in weights]
        + [pool, pltpu.SemaphoreType.DMA((12,))],
        compiler_params=params,
        name="project",
    )(*place(given, HBM))
    small = past + [
        input_filter_taps,
        write_filter_taps,
        read_filter_taps,
        step_size_bias,
        log_decay_rate,
        direct_path_gain,
        jnp.swapaxes(position_log_decay, 1, 2),
        grouped_norm_gain,
    ]
    tables, held, weight, gain, stream, split = pl.pallas_call(
        functools.partial(table_kernel, dims),
        out_shape=[
            pltpu.VMEM((layers, table_rows, LANES), f32),
            pltpu.VMEM(state.shape[1:], f32),
            pltpu.VMEM(output_matrix.shape[1:], bf16),
            pltpu.VMEM(input_norm_gain.shape, f32),
            pltpu.VMEM(hidden.shape, bf16),
            pltpu.VMEM((seqs * heads * state.shape[3], 2 * LANES), bf16),
        ],
        in_specs=[full(pltpu.SMEM), full()] + [full(HBM)] * (len(small) + 4),
        out_specs=[full()] * 6,
        scratch_shapes=[pltpu.VMEM(a.shape, a.dtype) for a in small]
        + [pltpu.VMEM((heads, LANES), f32), pltpu.SemaphoreType.DMA((len(small) + 4,))],
        compiler_params=params,
        cost_estimate=cost(4_000_000, 1_000_000),
        name="tables",
    )(
        lengths,
        *place([made[0]], VMEM),
        *place(small + [state, output_matrix, input_norm_gain, hidden], HBM),
    )
    states = None
    new_rows = []
    for layer in range(layers):
        parts = [made[0]] + [swap(made[mask], "dp", mask) for mask in range(1, fan)]
        if layer > 0:
            held, weight, split = fetch_state(layer, made[0])
        gated, row_values, *factors = mix(layer, parts, tables, split)
        new_rows.append(row_values)
        parts = swaps(gated, "dp")
        states = update(layer, factors, held, states)
        own = output(parts, weight, states)
        if lax.axis_size("tp") == 4:
            rounds = LINE_LAST if layer + 1 == layers else LINE
            partial = line_swaps(own, "tp", rounds)
        else:
            partial = swaps(own, "tp")
        if layer + 1 < layers:
            ahead = fetch(own, [(w, layer + 1) for w in weights])
            stream, *made = pl.pallas_call(
                functools.partial(next_project_kernel, dims, layer + 1),
                out_shape=[pltpu.VMEM(hidden.shape, bf16)] + [message] * fan,
                in_specs=[full()] * (2 + len(partial) + len(weights)),
                out_specs=[full()] * (1 + fan),
                scratch_shapes=[pool],
                compiler_params=params,
                name="project",
            )(*place([stream, *partial, gain, *ahead], VMEM))
    buffers = pl.pallas_call(
        functools.partial(buffer_kernel, dims, layers),
        out_shape=[jax.ShapeDtypeStruct(h.shape, bf16) for h in past],
        in_specs=[full()] * (1 + layers) + [full(HBM)] * 3,
        out_specs=[full(HBM)] * 3,
        scratch_shapes=[pltpu.VMEM(h.shape, bf16) for h in past] * 2 + [pltpu.SemaphoreType.DMA((3,))],
        compiler_params=params,
        cost_estimate=cost(4_000_000, 1_000_000),
        name="buffers",
    )(*place([own] + new_rows, VMEM), *place(past, HBM))
    buffers = [jnp.swapaxes(b, 1, 2) for b in buffers]
    stream = pl.pallas_call(
        close_kernel,
        out_shape=jax.ShapeDtypeStruct(hidden.shape, bf16),
        in_specs=[full()] * (1 + len(partial)),
        out_specs=full(),
        compiler_params=params,
        name="close",
    )(*place([stream, *partial], VMEM))
    return (stream, states, *buffers)


def kernels_fit(state, taps, write_taps, hidden, output_matrix, step_matrix):
    _, seqs, heads, head_dim, state_dim = state.shape
    shared = write_taps.shape[2] // LANES
    chunks = taps.shape[2] // LANES
    return (
        direct("dp")
        and direct("tp")
        and state_dim == LANES
        and head_dim * 2 == LANES
        and shared > 0
        and heads == 4 * shared
        and chunks == 2 * shared
        and chunks % 8 == 0
        and heads % 16 == 0
        and seqs * chunks <= LANES
        and seqs * chunks % 16 == 0
        and hidden.shape[0] == seqs * lax.axis_size("dp")
        and hidden.shape[0] % 8 == 0
        and hidden.shape[1] % LANES == 0
        and output_matrix.shape[2] % LANES == 0
        and step_matrix.shape[2] <= LANES
        and heads <= LANES // 2
    )


def convolve(buffer, new_row, weights, tap_valid):
    tap_rows = weights.astype(jnp.float32)
    depth = weights.shape[0] - 1
    summed = new_row.astype(jnp.float32) * tap_rows[depth]
    for k in range(depth):
        summed = summed + buffer[:, k].astype(jnp.float32) * tap_rows[k] * tap_valid[:, k : k + 1]
    shifted = jnp.concatenate([buffer[:, 1:], new_row[:, None]], axis=1)
    return (jax.nn.silu(summed), shifted)


def spread_groups(rows, seq_local, groups_local, per_group, state_dim):
    grouped = rows.reshape(seq_local, groups_local, 1, state_dim)
    return jnp.broadcast_to(grouped, (seq_local, groups_local, per_group, state_dim)).reshape(
        seq_local, groups_local * per_group, state_dim
    )


def exchange_rows(rows, axis, count):
    if not direct(axis):
        return lax.psum_scatter(rows, axis, scatter_dimension=0, tiled=True)
    me = lax.axis_index(axis)
    parts = [
        lax.dynamic_slice_in_dim(rows, (me ^ mask) * count, count, 0)
        for mask in range(lax.axis_size(axis))
    ]
    return tree_sum([parts[0]] + [swap(parts[mask], axis, mask) for mask in range(1, len(parts))])


def gather_rows(rows, axis):
    if not direct(axis):
        return lax.all_gather(rows, axis, axis=0, tiled=True)
    me, size = lax.axis_index(axis), lax.axis_size(axis)
    parts = [rows] + [swap(rows, axis, mask) for mask in range(1, size)]
    whole = jnp.zeros((size,) + rows.shape, rows.dtype)
    for mask in range(size):
        whole = lax.dynamic_update_index_in_dim(whole, parts[mask], me ^ mask, 0)
    return whole.reshape((size * rows.shape[0],) + rows.shape[1:])


def sum_copies(rows, axis):
    if not direct(axis):
        return lax.psum(rows, axis)
    return tree_sum([rows] + [swap(rows, axis, mask) for mask in range(1, lax.axis_size(axis))])


def on_device_plain(
    hidden,
    lengths,
    input_norm_gain,
    gate_matrix,
    input_matrix,
    write_matrix,
    read_matrix,
    step_matrix,
    step_size_bias,
    log_decay_rate,
    direct_path_gain,
    input_filter_taps,
    write_filter_taps,
    read_filter_taps,
    position_log_decay,
    grouped_norm_gain,
    output_matrix,
    recurrent_head_state,
    history_input_rows,
    history_write_rows,
    history_read_rows,
):
    seq_local = lengths.shape[0]
    heads_local = step_size_bias.shape[1]
    head_dim = recurrent_head_state.shape[3]
    state_dim = recurrent_head_state.shape[4]
    groups_local = write_filter_taps.shape[2] // state_dim
    per_group = heads_local // groups_local
    inner_local = heads_local * head_dim
    shared_local = groups_local * state_dim
    depth = input_filter_taps.shape[1] - 1
    token_position = lengths - 1
    tap_valid = (jnp.arange(depth)[None, :] >= depth - token_position[:, None]).astype(jnp.float32)
    state_is_valid = (token_position > 0).astype(jnp.float32)[:, None]
    position_indicator = (
        token_position[:, None] == jnp.arange(position_log_decay.shape[1])[None, :]
    ).astype(jnp.float32)
    head_first = lax.axis_index("tp") * heads_local
    stream = hidden
    states, values, writes, reads = ([], [], [], [])
    for layer_index in range(input_norm_gain.shape[0]):
        stream_float = stream.astype(jnp.float32)
        squares = jnp.sum(stream_float * stream_float, axis=1)
        normed = (stream_float * input_norm_gain[layer_index]).astype(jnp.bfloat16)
        pieces = [
            jnp.dot(normed, weight[layer_index], preferred_element_type=jnp.float32)
            for weight in (gate_matrix, input_matrix, write_matrix, read_matrix)
        ]
        step_term = jnp.dot(normed, step_matrix[layer_index], preferred_element_type=jnp.float32)
        heads_all = step_term.shape[1]
        width = sum(piece.shape[1] for piece in pieces)
        joined = jnp.concatenate(pieces + [step_term, squares[:, None]], axis=1)
        joined_mine = exchange_rows(joined, "dp", seq_local)
        mean_square = joined_mine[:, width + heads_all :] / D
        row_scale = lax.rsqrt(mean_square + epsilon)
        step_mine = joined_mine[:, width : width + heads_all]
        step_raw = lax.dynamic_slice_in_dim(step_mine, head_first, heads_local, 1) * row_scale
        scaled = joined_mine[:, :width] * row_scale
        proj_gate = scaled[:, :inner_local]
        value_row = scaled[:, inner_local : 2 * inner_local].astype(jnp.bfloat16)
        write_row = scaled[:, 2 * inner_local : 2 * inner_local + shared_local].astype(jnp.bfloat16)
        read_row = scaled[:, 2 * inner_local + shared_local :].astype(jnp.bfloat16)
        value_act, value_buf = convolve(
            history_input_rows[layer_index], value_row, input_filter_taps[layer_index], tap_valid
        )
        write_act, write_buf = convolve(
            history_write_rows[layer_index], write_row, write_filter_taps[layer_index], tap_valid
        )
        read_act, read_buf = convolve(
            history_read_rows[layer_index], read_row, read_filter_taps[layer_index], tap_valid
        )
        head_step_size = jax.nn.softplus(step_raw + step_size_bias[layer_index])
        current_log_decay = jnp.dot(
            position_indicator, position_log_decay[layer_index], precision=lax.Precision.HIGHEST
        )
        current_decay = (
            jnp.exp(-jnp.exp(log_decay_rate[layer_index]) * head_step_size + current_log_decay)
            * state_is_valid
        )
        value_heads = value_act.reshape(seq_local, heads_local, head_dim)
        write_heads = spread_groups(write_act, seq_local, groups_local, per_group, state_dim)
        read_heads = spread_groups(read_act, seq_local, groups_local, per_group, state_dim)
        updated = (
            current_decay[:, :, None, None] * recurrent_head_state[layer_index]
            + (head_step_size[:, :, None] * value_heads)[:, :, :, None] * write_heads[:, :, None, :]
        )
        readout = jnp.einsum("shpn,shn->shp", updated, read_heads, precision=lax.Precision.HIGHEST)
        mixed_heads = (
            readout + direct_path_gain[layer_index][None, :, None] * value_heads
        ) * jax.nn.silu(proj_gate.reshape(seq_local, heads_local, head_dim))
        grouped = mixed_heads.reshape(seq_local, groups_local, per_group * head_dim)
        grouped = grouped * lax.rsqrt(jnp.mean(grouped * grouped, axis=2, keepdims=True) + epsilon)
        gated_rows = (
            grouped.reshape(seq_local, inner_local) * grouped_norm_gain[layer_index]
        ).astype(jnp.bfloat16)
        out_weight = output_matrix[layer_index]

        gathered = gather_rows(gated_rows, "dp")
        partial_out = jnp.dot(gathered, out_weight, preferred_element_type=jnp.float32)
        branch = sum_copies(partial_out, "tp")
        stream = (stream_float + branch).astype(jnp.bfloat16)
        states.append(updated)
        values.append(value_buf)
        writes.append(write_buf)
        reads.append(read_buf)
    return (stream, jnp.stack(states), jnp.stack(values), jnp.stack(writes), jnp.stack(reads))


def on_device(*args):
    hidden, taps, write_taps = args[0], args[11], args[12]
    if kernels_fit(args[17], taps, write_taps, hidden, args[16], args[7]):
        return on_device_kernels(*args)
    return on_device_plain(*args)


def solution(mesh):
    placed = (
        P("grp", "dp"),
        P(("grp", "dp")),
        P(None, "dp"),
        P(None, "dp", "tp"),
        P(None, "dp", "tp"),
        P(None, "dp", "tp"),
        P(None, "dp", "tp"),
        P(None, "dp", None),
        P(None, "tp"),
        P(None, "tp"),
        P(None, "tp"),
        P(None, None, "tp"),
        P(None, None, "tp"),
        P(None, None, "tp"),
        P(None, None, "tp"),
        P(None, "tp"),
        P(None, "tp", "dp"),
        P(None, ("grp", "dp"), "tp", None, None),
        P(None, ("grp", "dp"), None, "tp"),
        P(None, ("grp", "dp"), None, "tp"),
        P(None, ("grp", "dp"), None, "tp"),
    )
    return jax.shard_map(
        on_device,
        mesh=mesh,
        in_specs=placed,
        out_specs=(
            P("grp", "dp"),
            P(None, ("grp", "dp"), "tp", None, None),
            P(None, ("grp", "dp"), None, "tp"),
            P(None, ("grp", "dp"), None, "tp"),
            P(None, ("grp", "dp"), None, "tp"),
        ),
        check_vma=False,
    )
```
